256 devices in a mesh: sp: 32 (over z, y), tp: 8 (over x, core).
Axes of the slice: x: 4, y: 4, z: 8, core: 2. Of those that a mesh axis runs over, the one named last changes fastest.
Arguments:
- block_input: bfloat16 [32768, 2048], P('sp'), may hold values from -6 to 6
- value_proj: bfloat16 [2048, 1024], P(None, 'tp'), may hold values from -0.125 to 0.125
- gate_proj: bfloat16 [2048, 1024], P(None, 'tp'), may hold values from -0.125 to 0.125
- conv_taps: float32 [31, 1024], P(None, 'tp'), may hold values from -3 to 3
- norm_gain: float32 [1024], P('tp'), may hold values from 0.1 to 1.9
- out_proj: bfloat16 [2048, 1024], P(None, 'tp'), may hold values from -0.125 to 0.125
- grad_output: bfloat16 [32768, 2048], P('sp'), may hold values from -6 to 6
Outputs:
- input_grad: bfloat16 [32768, 2048], P('sp', 'tp')
- value_grad: float32 [2048, 1024], P('sp', 'tp')
- gate_grad: float32 [2048, 1024], P('sp', 'tp')
- out_grad: float32 [2048, 1024], P('sp', 'tp')
- taps_grad: float32 [31, 1024], P(None, 'tp')
- gain_grad: float32 [1024], P('tp')
The draws below stay inside these ranges and needn't reach their ends.
All inputs are finite; a program needn't handle non-finite values.
Results may differ from the reference program's by a relative error of at most 0.015.
Values may be sent and summed in bfloat16 or wider, within the bound.
No kernel may reach another device: no remote copies, remote signals or barrier semaphores. Data moves between devices by JAX's collectives and lax.ppermute only.
A program may use at most 64 MiB of HBM per device.

```python
import jax
import jax.numpy as jnp
from jax import lax

D = 2048
C = 1024
K = 31
TOKENS = 32768
N_TP = 8


def draw_conv_taps(key, part):
    base_key, order_key = jax.random.split(key)
    raw_taps = jnp.clip(jax.random.normal(base_key, (K, C), jnp.float32), -4.0, 4.0)
    group_order = jax.random.permutation(order_key, 8).astype(jnp.float32)
    group_index = jnp.arange(C) * 8 // C
    group_scale = 0.3 * 10.0 ** (group_order[group_index] / 7.0)
    return raw_taps * group_scale[None, :] / jnp.sqrt(jnp.float32(K))


def with_spikes(result, key, source, target, blocks, factor):
    def block_of(dim):
        return (jnp.arange(result.shape[dim]) // (result.shape[dim] // blocks)).reshape((-1,) + (1,) * (result.ndim - 1 - dim))

    one_side = jax.random.permutation(key, blocks)[block_of(target)]
    far = (block_of(target) + blocks // 2) % blocks
    return jnp.where((block_of(source) == one_side) | (block_of(source) == far), factor * result, result)


def block_scale(stream_key, shape, cuts, least, high):
    def one(axis_at, parts):
        heights = jax.random.uniform(jax.random.fold_in(jax.random.fold_in(stream_key, 6), axis_at), (parts,), jnp.float32, least / len(cuts), high / len(cuts))
        return jnp.repeat(jnp.exp(heights), shape[axis_at] // parts).reshape((-1,) + (1,) * (len(shape) - axis_at - 1))

    loudness = one(*cuts[0])
    for cut in cuts[1:]:
        loudness = loudness * one(*cut)
    return loudness


def normal_values(stream_key, dims, spread, reach, cuts=(), dtype=jnp.bfloat16):
    values = spread * jax.random.normal(stream_key, dims, jnp.float32)
    if cuts:
        values = values * block_scale(stream_key, dims, cuts, -0.22, 0.18)
    return jnp.clip(values, -reach, reach).astype(dtype)


def bell_draw_with(rng, shape, deviation, most, pieces, heavy, held_as=jnp.bfloat16):
    entries = deviation * jax.random.normal(rng, shape, jnp.float32)
    if pieces:
        entries = entries * block_scale(rng, shape, pieces, -0.22, 0.18)
    return jnp.clip(with_spikes(entries, jax.random.fold_in(rng, 3), *heavy), -most, most).astype(held_as)


def setup_inputs(seed: int = 0) -> dict:
    keys = jax.random.split(jax.random.key(seed), 8)
    block_input = bell_draw_with(keys[0], (TOKENS, D), 1.0, 6.0, ((0, 32),), (0, 1, 32, 2.75))
    value_proj = normal_values(keys[1], (D, C), D ** -0.5, 0.125, ((1, 8),))
    gate_proj = normal_values(keys[2], (D, C), D ** -0.5, 0.125, ((1, 8),))
    conv_taps = draw_conv_taps(jax.random.fold_in(keys[7], 71), 0)
    norm_gain = jnp.clip(1.0 + 0.18 * jax.random.normal(keys[4], (C,), jnp.float32), 0.1, 1.9)
    out_proj = normal_values(keys[5], (D, C), D ** -0.5, 0.125, ((1, 8),))
    grad_output = bell_draw_with(keys[6], (TOKENS, D), 1.0, 6.0, ((0, 32),), (0, 1, 32, 2.75))
    return dict(block_input=block_input, value_proj=value_proj, gate_proj=gate_proj, conv_taps=conv_taps, norm_gain=norm_gain, out_proj=out_proj, grad_output=grad_output)


norm_floor = 0.1

def reference(block_input, value_proj, gate_proj, conv_taps, norm_gain, out_proj, grad_output):
    value = jnp.dot(block_input, value_proj, preferred_element_type=jnp.float32)
    gate_raw = jnp.dot(block_input, gate_proj, preferred_element_type=jnp.float32)
    sgate = jax.nn.sigmoid(gate_raw)
    mixed = (value * sgate).astype(jnp.bfloat16)
    tap_count = conv_taps.shape[0]
    reach_rows = tap_count - 1
    seq_rows = mixed.shape[0]
    history = jnp.concatenate([jnp.zeros((reach_rows, C), jnp.bfloat16), mixed], axis=0)
    conv_out = jnp.zeros((seq_rows, C), jnp.float32)
    for tap_index in range(tap_count):
        offset = reach_rows - tap_index
        conv_out = conv_out + conv_taps[tap_index] * history[offset:offset + seq_rows].astype(jnp.float32)
    center = lax.optimization_barrier(jnp.sum(conv_out, axis=1)) / C
    squares = lax.optimization_barrier(jnp.sum(conv_out * conv_out, axis=1)) / C
    inverse = lax.rsqrt(squares - center * center + norm_floor)
    normed = (conv_out - center[:, None]) * inverse[:, None]
    scaled = normed * norm_gain
    squash = jax.nn.sigmoid(scaled)
    activated = (scaled * squash).astype(jnp.bfloat16)
    slope = jnp.dot(grad_output, out_proj, preferred_element_type=jnp.float32)
    pre_slope = slope * squash * (1.0 + scaled * (1.0 - squash))
    gain_grad = lax.optimization_barrier(jnp.sum(pre_slope * normed, axis=0))
    norm_slope = pre_slope * norm_gain
    slope_sum = lax.optimization_barrier(jnp.sum(norm_slope, axis=1)) / C
    cross_sum = lax.optimization_barrier(jnp.sum(norm_slope * normed, axis=1)) / C
    conv_slope = inverse[:, None] * (norm_slope - slope_sum[:, None] - normed * cross_sum[:, None])
    taps_list = []
    for tap_index in range(tap_count):
        offset = reach_rows - tap_index
        taps_list.append(lax.optimization_barrier(jnp.sum(conv_slope * history[offset:offset + seq_rows].astype(jnp.float32), axis=0)))
    taps_grad = jnp.stack(taps_list)
    future = jnp.concatenate([conv_slope, jnp.zeros((reach_rows, C), jnp.float32)], axis=0)
    mixed_slope = jnp.zeros((seq_rows, C), jnp.float32)
    for tap_index in range(tap_count):
        mixed_slope = mixed_slope + conv_taps[tap_index] * future[tap_index:tap_index + seq_rows]
    value_slope = (mixed_slope * sgate).astype(jnp.bfloat16)
    gate_slope = (mixed_slope * value * sgate * (1.0 - sgate)).astype(jnp.bfloat16)
    value_grad = jnp.dot(block_input.T, value_slope, preferred_element_type=jnp.float32)
    gate_grad = jnp.dot(block_input.T, gate_slope, preferred_element_type=jnp.float32)
    out_grad = jnp.dot(grad_output.T, activated, preferred_element_type=jnp.float32)
    group_width = C // N_TP
    running = jnp.zeros((seq_rows, D), jnp.float32)
    for group_index in range(N_TP):
        first_col = group_index * group_width
        last_col = first_col + group_width
        partial_value = jnp.dot(value_slope[:, first_col:last_col], value_proj[:, first_col:last_col].T, preferred_element_type=jnp.float32)
        partial_value = partial_value + jnp.dot(gate_slope[:, first_col:last_col], gate_proj[:, first_col:last_col].T, preferred_element_type=jnp.float32)
        rounded = lax.optimization_barrier(partial_value.astype(jnp.bfloat16))
        running = running + rounded.astype(jnp.float32)
    input_grad = running.astype(jnp.bfloat16)
    return (input_grad, value_grad, gate_grad, out_grad, taps_grad, gain_grad)
```

```python
import jax
import jax.numpy as jnp
from jax import lax
from jax.experimental import pallas as pl
from jax.experimental.pallas import tpu as pltpu
from jax.sharding import Mesh
from jax.sharding import PartitionSpec as P

SP = ("z", "y")
TP = ("x", "c")
NZ, NY, NX, NC = 8, 4, 4, 2
C = 1024
D = 2048
K = 31
ROWS = 1024
W = 128
PAD = 32
EXT = ROWS + PAD
TAIL = 16
FLOOR = 0.1
F32 = jnp.float32
BF16 = jnp.bfloat16
EXACT = lax.Precision.HIGHEST


def params(mib, **more):
    return pltpu.CompilerParams(vmem_limit_bytes=mib * 1024 * 1024, **more)


def cost(flops, size):
    return pl.CostEstimate(flops=flops, bytes_accessed=size, transcendentals=0)


def whole(shape):
    return pl.BlockSpec(shape, lambda *_: (0,) * len(shape))


def dot(a, b):
    return jnp.dot(a, b, preferred_element_type=F32)


def shape_of(shape, dtype=F32):
    return jax.ShapeDtypeStruct(shape, dtype)


def edge_kernel(head, tail, grad_head, value_proj, gate_proj, out_proj, to_next, to_prior):
    def mixed_of(rows):
        value = dot(rows, value_proj[...])
        return (value * jax.nn.sigmoid(dot(rows, gate_proj[...]))).astype(BF16).astype(F32)

    mixed = mixed_of(jnp.concatenate([head[...], tail[...]], axis=0))
    to_prior[:PAD] = mixed[:PAD]
    to_next[...] = mixed[PAD:]
    to_prior[PAD:] = dot(grad_head[...], out_proj[...])


def edges(block_input, grad_output, value_proj, gate_proj, out_proj):
    first = pl.BlockSpec((PAD, D), lambda i: (0, 0))
    last = pl.BlockSpec((PAD, D), lambda i: (ROWS // PAD - 1, 0))
    proj = whole((D, W))
    return pl.pallas_call(
        edge_kernel,
        grid=(1,),
        in_specs=[first, last, first, proj, proj, proj],
        out_specs=[whole((PAD, W)), whole((2 * PAD, W))],
        out_shape=[shape_of((PAD, W)), shape_of((2 * PAD, W))],
        compiler_params=params(12),
        cost_estimate=cost(2 * 96 * D * 256, 2 * 1024 * 1024),
    )(block_input, block_input, grad_output, value_proj, gate_proj, out_proj)


def glu_kernel(rows, value_proj, gate_proj, mixed, sgate, factor, both):
    @pl.when(pl.program_id(0) == 0)
    def _():
        both[:, :W] = value_proj[...]
        both[:, W:] = gate_proj[...]

    parts = dot(rows[...], both[...])
    value = parts[:, :W]
    gate = jax.nn.sigmoid(parts[:, W:])
    mixed[...] = (value * gate).astype(BF16).astype(F32)
    sgate[...] = gate
    factor[...] = value * gate * (1.0 - gate)


def glu(block_input, value_proj, gate_proj, step=128):
    out = pl.BlockSpec((step, W), lambda i: (i, 0))
    return pl.pallas_call(
        glu_kernel,
        grid=(ROWS // step,),
        in_specs=[pl.BlockSpec((step, D), lambda i: (i, 0)), whole((D, W)), whole((D, W))],
        out_specs=[out, out, out],
        out_shape=[shape_of((ROWS, W))] * 3,
        scratch_shapes=[pltpu.VMEM((D, 2 * W), BF16)],
        compiler_params=params(12),
        cost_estimate=cost(2 * ROWS * D * 256, 7 * 1024 * 1024),
    )(block_input, value_proj, gate_proj)


def slope_kernel(rows, out_proj, slope):
    slope[...] = dot(rows[...], out_proj[...])


def slopes_of(grad_output, out_proj, step=128):
    return pl.pallas_call(
        slope_kernel,
        grid=(ROWS // step,),
        in_specs=[pl.BlockSpec((step, D), lambda i: (i, 0)), whole((D, W))],
        out_specs=pl.BlockSpec((step, W), lambda i: (i, 0)),
        out_shape=shape_of((ROWS, W)),
        compiler_params=params(12),
        cost_estimate=cost(2 * ROWS * D * 256, 5 * 1024 * 1024),
    )(grad_output, out_proj)


def row_sums(value):
    return lax.dot_general(
        jnp.ones((8, W), F32), value, (((1,), (1,)), ((), ())), precision=EXACT, preferred_element_type=F32
    )


def spread_sums(rows):
    return lax.dot_general(
        rows, jnp.ones((8, W), F32), (((0,), (0,)), ((), ())), precision=EXACT, preferred_element_type=F32
    )


def conv_kernel(mixed, prior, after, taps, history, conv, sums):
    history[:PAD] = prior[...]
    history[PAD : PAD + ROWS] = mixed[...]
    history[PAD + ROWS :] = after[:PAD]
    step = 96

    def body(i, carry):
        base = pl.multiple_of(i * step, step)
        total = jnp.zeros((step, W), F32)
        for k in range(K):
            total = total + taps[k : k + 1, :] * history[pl.ds(base + (PAD - k), step), :]
        conv[pl.ds(base, step), :] = total
        return carry

    lax.fori_loop(0, EXT // step, body, 0)
    value = conv[...]
    sums[:, 0, :] = row_sums(value)
    sums[:, 1, :] = row_sums(value * value)


def conv_of(mixed, prior, after, taps):
    return pl.pallas_call(
        conv_kernel,
        out_shape=[shape_of((EXT + PAD, W)), shape_of((EXT, W)), shape_of((8, 2, EXT))],
        compiler_params=params(16),
        cost_estimate=cost(2 * ROWS * D * 128, 2 * 1024 * 1024),
    )(mixed, prior, after, taps)


def norm_kernel(conv, slope, after, gain, sums, normed, norm_slope, inverse, activated, back, gain_part):
    center = spread_sums(sums[:, 0, :]) / C
    squares = spread_sums(sums[:, 1, :]) / C
    inv = lax.rsqrt(squares - center * center + FLOOR)
    norm = (conv[...] - center) * inv
    inverse[...] = inv
    normed[...] = norm
    scale = gain[...]
    scaled = norm * scale
    squash = jax.nn.sigmoid(scaled)
    activated[...] = (scaled * squash)[:ROWS].astype(BF16)
    bend = squash * (1.0 + scaled * (1.0 - squash))
    own = slope[...] * bend[:ROWS]
    gain_part[...] = jnp.sum(own * norm[:ROWS], axis=0, keepdims=True)
    own = own * scale
    past = after[PAD:] * bend[ROWS:] * scale
    norm_slope[:ROWS] = own
    norm_slope[ROWS:] = past
    value = norm_slope[...]
    back[:, 0, :] = row_sums(value)
    back[:, 1, :] = row_sums(value * norm)


def norm_of(conv, slope, after, gain, sums):
    ext = shape_of((EXT, W))
    return pl.pallas_call(
        norm_kernel,
        out_shape=[ext, ext, ext, shape_of((ROWS, W), BF16), shape_of((8, 2, EXT)), shape_of((1, W))],
        compiler_params=params(24),
        cost_estimate=cost(2 * ROWS * D * 128, 2 * 1024 * 1024),
    )(conv, slope, after, gain, sums)


def adjoint_kernel(
    last, normed, norm_slope, inverse, back, history, taps, sgate, factor, gain_part, slopes, taps_part, curve
):
    slope_sum = spread_sums(back[:, 0, :]) / C
    cross_sum = spread_sums(back[:, 1, :]) / C
    curve[...] = inverse[...] * (norm_slope[...] - slope_sum - normed[...] * cross_sum)

    @pl.when(last[0] == 1)
    def _():
        curve[ROWS:] = jnp.zeros((PAD, W), F32)

    step = 128

    def spread(i, carry):
        base = pl.multiple_of(i * step, step)
        total = jnp.zeros((step, W), F32)
        for k in range(K):
            total = total + taps[k : k + 1, :] * curve[pl.ds(base + k, step), :]
        slopes[pl.ds(base, step), :W] = (total * sgate[pl.ds(base, step), :]).astype(BF16)
        slopes[pl.ds(base, step), W:] = (total * factor[pl.ds(base, step), :]).astype(BF16)
        return carry

    lax.fori_loop(0, ROWS // step, spread, 0)

    inner = 32

    def gather(i, sums):
        base = pl.multiple_of(i * inner, inner)
        now = curve[pl.ds(base, inner), :]
        out = []
        for k in range(K):
            term = now * history[pl.ds(base + (PAD - k), inner), :]
            term = (term[:8] + term[8:16]) + (term[16:24] + term[24:])
            out.append(sums[k] + term)
        return tuple(out)

    sums = lax.fori_loop(0, ROWS // inner, gather, tuple(jnp.zeros((8, W), F32) for _ in range(K)))
    for k in range(K):
        taps_part[k : k + 1, :] = jnp.sum(sums[k], axis=0, keepdims=True)
    taps_part[K:, :] = gain_part[...]


def adjoint_of(last, normed, norm_slope, inverse, back, history, taps, sgate, factor, gain_part):
    vmem = pl.BlockSpec(memory_space=pltpu.VMEM)
    return pl.pallas_call(
        adjoint_kernel,
        in_specs=[pl.BlockSpec(memory_space=pltpu.SMEM)] + [vmem] * 9,
        out_shape=[shape_of((ROWS, 2 * W), BF16), shape_of((K + 1, W))],
        scratch_shapes=[pltpu.VMEM((EXT, W), F32)],
        compiler_params=params(24),
        cost_estimate=cost(2 * ROWS * D * 256, 2 * 1024 * 1024),
    )(last, normed, norm_slope, inverse, back, history, taps, sgate, factor, gain_part)


def out_grad_kernel(cols, activated, out, side):
    @pl.when(pl.program_id(0) == 0)
    def _():
        side[...] = activated[...].T

    part = dot(side[...], cols[...])
    out[...] = part.T.astype(BF16).reshape(NY, D // 32, W)


def out_grad_of(grad_output, activated):
    step = D // NZ
    return pl.pallas_call(
        out_grad_kernel,
        grid=(NZ,),
        in_specs=[pl.BlockSpec((ROWS, step), lambda i: (0, i)), whole((ROWS, W))],
        out_specs=pl.BlockSpec((NY, D // 32, W), lambda i: (0, i, 0)),
        out_shape=shape_of((NY, D // NY, W), BF16),
        scratch_shapes=[pltpu.VMEM((W, ROWS), BF16)],
        compiler_params=params(12),
        cost_estimate=cost(2 * ROWS * D * 256, 5 * 1024 * 1024),
    )(grad_output, activated)


def weight_grad_kernel(cols, slopes, out_part, taps_part, out, side):
    i = pl.program_id(0)

    @pl.when(i == 0)
    def _():
        side[...] = slopes[...].T
        small = taps_part[...].astype(BF16)
        block = jnp.concatenate([small[:16], small[16:], jnp.zeros((16, W), BF16)], axis=1)
        for y in range(NY):
            out[y, D // NY :, :] = block

    part = dot(side[...], cols[...])
    part = part.T.astype(BF16).reshape(NY, D // 32, 2 * W)
    at = pl.multiple_of(i * (D // 32), D // 32)
    out[:, pl.ds(at, D // 32), : 2 * W] = part
    out[:, pl.ds(at, D // 32), 2 * W :] = out_part[...]


def weight_grad_of(block_input, slopes, out_part, taps_part):
    step = D // NZ
    full = (NY, D // NY + TAIL, 3 * W)
    return pl.pallas_call(
        weight_grad_kernel,
        grid=(NZ,),
        in_specs=[
            pl.BlockSpec((ROWS, step), lambda i: (0, i)),
            whole((ROWS, 2 * W)),
            pl.BlockSpec((NY, D // 32, W), lambda i: (0, i, 0)),
            whole((K + 1, W)),
        ],
        out_specs=whole(full),
        out_shape=shape_of(full, BF16),
        scratch_shapes=[pltpu.VMEM((2 * W, ROWS), BF16)],
        compiler_params=params(16),
        cost_estimate=cost(2 * ROWS * D * 256, 7 * 1024 * 1024),
    )(block_input, slopes, out_part, taps_part)


def middle_kernel(arrived, out):
    total = arrived[0].astype(F32)
    for y in range(1, NY):
        total = total + arrived[y].astype(F32)
    total = total.astype(BF16)
    out[:, : D // 32, :] = total[: D // NY].reshape(NZ, D // 32, 3 * W)
    for z in range(NZ):
        out[z, D // 32 :, :] = total[D // NY :]


def middle_of(arrived):
    return pl.pallas_call(
        middle_kernel,
        out_shape=shape_of((NZ, D // 32 + TAIL, 3 * W), BF16),
        compiler_params=params(12),
        cost_estimate=cost(2 * ROWS * D, 2 * 1024 * 1024),
    )(arrived)


def final_kernel(arrived, value_grad, gate_grad, out_grad, taps_grad, gain_grad):
    total = arrived[0].astype(F32)
    for z in range(1, NZ):
        total = total + arrived[z].astype(F32)
    value_grad[...] = total[: D // 32, :W]
    gate_grad[...] = total[: D // 32, W : 2 * W]
    out_grad[...] = total[: D // 32, 2 * W :]
    taps_grad[:16] = total[D // 32 :, :W]
    taps_grad[16:] = total[D // 32 : D // 32 + 15, W : 2 * W]
    gain_grad[...] = total[D // 32 + 15 :, W : 2 * W]


def final_of(arrived):
    part = shape_of((D // 32, W))
    return pl.pallas_call(
        final_kernel,
        out_shape=[part, part, part, shape_of((K, W)), shape_of((1, W))],
        compiler_params=params(12),
        cost_estimate=cost(2 * ROWS * D, 1024 * 1024),
    )(arrived)


def input_grad_kernel(*refs):
    *sides, out = refs
    half = ROWS // 2
    total = None
    blocks, weights = sides[:10], sides[10:]
    pieces = [(b, w) for b, w in zip(blocks[:6], [0, 1, 2, 3, 4, 5])]
    step = 256
    for r in range(0, ROWS, step):
        total = jnp.zeros((step, D // 8), F32)
        for slot in range(8):
            if slot < 6:
                rows = blocks[slot][r : r + step, :]
            else:
                low, high = blocks[6 + 2 * (slot - 6)], blocks[7 + 2 * (slot - 6)]
                rows = low[r : r + step, :] if r < half else high[r - half : r - half + step, :]
            total = total + lax.dot_general(
                rows[:, :W], weights[2 * slot][...], (((1,), (1,)), ((), ())), preferred_element_type=F32
            )
            total = total + lax.dot_general(
                rows[:, W:], weights[2 * slot + 1][...], (((1,), (1,)), ((), ())), preferred_element_type=F32
            )
        out[r : r + step, :] = total.astype(BF16)


def input_grad_of(blocks, weights):
    return pl.pallas_call(
        input_grad_kernel,
        out_shape=shape_of((ROWS, D // 8), BF16),
        compiler_params=params(32),
        cost_estimate=cost(2 * ROWS * D * 512, 6 * 1024 * 1024),
    )(*blocks, *weights)


def along(value, axis, by):
    count = lax.axis_size(axis)
    return lax.ppermute(value, axis, [(i, (i + by) % count) for i in range(count)])


def from_behind(value, by):
    count = lax.axis_size(SP)
    return lax.ppermute(value, SP, [(i, i + by) for i in range(count) if 0 <= i + by < count])


def gathered(own):
    half = ROWS // 2
    other = along(own, "c", 1)
    behind = along(own, "x", 1)
    ahead = along(own, "x", -1)
    far_low = along(behind[:half], "x", 1)
    far_high = along(ahead[half:], "x", -1)
    return [own, other, behind, along(behind, "c", 1), ahead, along(ahead, "c", 1),
            far_low, far_high, along(far_low, "c", 1), along(far_high, "c", 1)]


def weights_gathered(value_proj, gate_proj):
    here = lax.axis_index("x")
    core = lax.axis_index("c")
    both = jnp.stack([value_proj, gate_proj]).reshape(2, NX, NC, D // 8, W)
    mine = lax.dynamic_index_in_dim(both, core, 2, keepdims=False)
    theirs = along(lax.dynamic_index_in_dim(both, 1 - core, 2, keepdims=False), "c", 1)
    pair = jnp.stack([mine, theirs])

    def sent(by):
        piece = lax.dynamic_index_in_dim(pair, (here + by) % NX, 2, keepdims=False)
        return along(piece, "x", by) if by else piece

    out = []
    for piece in (sent(0), sent(1), sent(-1), sent(2)):
        for c in range(2):
            out += [piece[c, 0], piece[c, 1]]
    return out


def shards(block_input, value_proj, gate_proj, conv_taps, norm_gain, out_proj, grad_output):
    to_next, to_prior = edges(block_input, grad_output, value_proj, gate_proj, out_proj)
    prior = from_behind(to_next, 1)
    after = from_behind(to_prior, -1)
    mixed, sgate, factor = glu(block_input, value_proj, gate_proj)
    history, conv, sums = conv_of(mixed, prior, after, conv_taps)
    sums = lax.all_to_all(sums, TP, 0, 0, tiled=True)
    slope = slopes_of(grad_output, out_proj)
    normed, norm_slope, inverse, activated, back, gain_part = norm_of(
        conv, slope, after, norm_gain.reshape(1, W), sums
    )
    back = lax.all_to_all(back, TP, 0, 0, tiled=True)
    out_part = out_grad_of(grad_output, activated)
    last = (lax.axis_index(SP) == NZ * NY - 1).astype(jnp.int32).reshape(1)
    slopes, taps_part = adjoint_of(
        last, normed, norm_slope, inverse, back, history, conv_taps, sgate, factor, gain_part
    )
    blocks = gathered(slopes)
    partial = weight_grad_of(block_input, slopes, out_part, taps_part)
    partial = lax.all_to_all(partial, "y", 0, 0, tiled=True)
    weights = weights_gathered(value_proj, gate_proj)
    input_grad = input_grad_of(blocks, weights)
    partial = lax.all_to_all(middle_of(partial), "z", 0, 0, tiled=True)
    value_grad, gate_grad, out_grad, taps_grad, gain_grad = final_of(partial)
    return (input_grad, value_grad, gate_grad, out_grad, taps_grad, gain_grad.reshape(W))


def solution(mesh):
    finer = Mesh(mesh.devices.reshape(NZ, NY, NX, NC), ("z", "y", "x", "c"))
    placed = (P(SP, None), P(None, TP), P(None, TP), P(None, TP), P(TP), P(None, TP), P(SP, None))
    split = P(SP, TP)
    return jax.shard_map(
        shards,
        mesh=finer,
        in_specs=placed,
        out_specs=(split, split, split, split, P(None, TP), P(TP)),
        check_vma=False,
    )
```

```python
import jax
import jax.numpy as jnp
from jax import lax
from jax.experimental import pallas as pl
from jax.experimental.pallas import tpu as pltpu
from jax.sharding import Mesh
from jax.sharding import PartitionSpec as P

SP = ("z", "y")
TP = ("x", "c")
NZ, NY, NX, NC = 8, 4, 4, 2
C = 1024
D = 2048
K = 31
ROWS = 1024
W = 128
PAD = 32
EXT = ROWS + PAD
TAIL = 16
FLOOR = 0.1
F32 = jnp.float32
BF16 = jnp.bfloat16
EXACT = lax.Precision.HIGHEST


def params(mib, **more):
    return pltpu.CompilerParams(vmem_limit_bytes=mib * 1024 * 1024, **more)


def cost(flops, size):
    return pl.CostEstimate(flops=flops, bytes_accessed=size, transcendentals=0)


def whole(shape):
    return pl.BlockSpec(shape, lambda *_: (0,) * len(shape))


def dot(a, b):
    return jnp.dot(a, b, preferred_element_type=F32)


def shape_of(shape, dtype=F32):
    return jax.ShapeDtypeStruct(shape, dtype)


def edge_kernel(rows, grads, value_proj, gate_proj, out_proj, to_next, to_prior, both, out_side, *rest):
    parts, (ends, grad_head, sems, part_sems) = rest[:8], rest[8:]
    here = lax.axis_index("x")
    core = lax.axis_index("c")
    pairs = [
        (rows.at[:PAD], ends.at[:PAD]),
        (rows.at[ROWS - PAD :], ends.at[PAD:]),
        (value_proj, both.at[:, :W]),
        (gate_proj, both.at[:, W:]),
        (grads.at[:PAD], grad_head),
        (out_proj, out_side),
    ]
    copies = [pltpu.make_async_copy(a, b, sems.at[i]) for i, (a, b) in enumerate(pairs)]
    for copy in copies:
        copy.start()
    for copy in copies[:4]:
        copy.wait()
    cuts = []
    for slot in range(8):
        dest = lax.rem(here + slot // 2, NX) * NC + (core if slot % 2 == 0 else 1 - core)
        at = pl.multiple_of(dest * (D // 8), D // 8)
        cuts.append(pltpu.make_async_copy(both.at[pl.ds(at, D // 8), :], parts[slot], part_sems.at[slot]))
        cuts[-1].start()
    both_parts = dot(ends[...], both[...])
    mixed = (both_parts[:, :W] * jax.nn.sigmoid(both_parts[:, W:])).astype(BF16).astype(F32)
    to_prior[:PAD] = mixed[:PAD]
    to_next[...] = mixed[PAD:]
    for copy in copies[4:]:
        copy.wait()
    to_prior[PAD:] = dot(grad_head[...], out_side[...])
    for cut in cuts:
        cut.wait()


def in_hbm(value):
    return pltpu.with_memory_space_constraint(value, pltpu.HBM)


def edges(block_input, grad_output, value_proj, gate_proj, out_proj):
    hbm = pl.BlockSpec(memory_space=pltpu.HBM)
    vmem = pl.BlockSpec(memory_space=pltpu.VMEM)
    args = [in_hbm(v) for v in (block_input, grad_output, value_proj, gate_proj, out_proj)]
    return pl.pallas_call(
        edge_kernel,
        in_specs=[hbm] * 5,
        out_specs=[vmem] * 4 + [hbm] * 8,
        out_shape=[shape_of((PAD, W)), shape_of((2 * PAD, W)), shape_of((D, 2 * W), BF16), shape_of((D, W), BF16)]
        + [shape_of((D // 8, 2 * W), BF16)] * 8,
        scratch_shapes=[
            pltpu.VMEM((2 * PAD, D), BF16),
            pltpu.VMEM((PAD, D), BF16),
            pltpu.SemaphoreType.DMA((6,)),
            pltpu.SemaphoreType.DMA((8,)),
        ],
        compiler_params=params(8),
        cost_estimate=cost(2 * 96 * D * 256, 2 * 1024 * 1024),
    )(*args)


def glu_kernel(rows, both, mixed, sgate, factor):
    step = 256
    for r in range(0, ROWS, step):
        parts = dot(rows[r : r + step, :], both[...])
        value = parts[:, :W]
        gate = jax.nn.sigmoid(parts[:, W:])
        mixed[r : r + step, :] = (value * gate).astype(BF16).astype(F32)
        sgate[r : r + step, :] = gate
        factor[r : r + step, :] = value * gate * (1.0 - gate)


def glu(block_input, both):
    return pl.pallas_call(
        glu_kernel,
        out_shape=[shape_of((ROWS, W))] * 3,
        compiler_params=params(12),
        cost_estimate=cost(2 * ROWS * D * 256, 7 * 1024 * 1024),
    )(block_input, both)


def slope_kernel(rows, out_side, slope):
    slope[...] = dot(rows[...], out_side[...])


def slopes_of(grad_output, out_side):
    return pl.pallas_call(
        slope_kernel,
        out_shape=shape_of((ROWS, W)),
        compiler_params=params(8),
        cost_estimate=cost(2 * ROWS * D * 256, 5 * 1024 * 1024),
    )(grad_output, out_side)


def store_sums(out, value, other):
    out[0, :] = jnp.sum(value, axis=1)
    out[1, :] = jnp.sum(other, axis=1)


def spread_sums(parts, outs):
    total = (parts[0][...] + parts[1][...]) + (parts[2][...] + parts[3][...])
    step = 96
    for row, out in enumerate(outs):
        mean = total[row : row + 1, :] * (1.0 / C)
        for r in range(0, EXT, step):
            out[r : r + step, :] = jnp.broadcast_to(mean[:, r : r + step], (W, step)).T


def swept(source, taps, base, step, shifts):
    total = jnp.zeros((step, W), F32)
    for residue in range(8):
        ks = [k for k in range(K) if shifts(k) % 8 == residue]
        low = min(shifts(k) for k in ks)
        high = max(shifts(k) for k in ks)
        block = source[pl.ds(base + low, step + high - low), :]
        for k in ks:
            at = shifts(k) - low
            total = total + taps[k : k + 1, :] * block[at : at + step]
    return total


def conv_kernel(mixed, prior, after, taps, history, conv, sums):
    history[:PAD] = prior[...]
    history[PAD : PAD + ROWS] = mixed[...]
    history[PAD + ROWS :] = after[:PAD]
    step = 96

    def body(i, carry):
        base = pl.multiple_of(i * step, step)
        conv[pl.ds(base, step), :] = swept(history, taps, base, step, lambda k: PAD - k)
        return carry

    lax.fori_loop(0, EXT // step, body, 0)
    value = conv[...]
    store_sums(sums, value, value * value)


def conv_of(mixed, prior, after, taps):
    return pl.pallas_call(
        conv_kernel,
        out_shape=[shape_of((EXT + PAD, W)), shape_of((EXT, W)), shape_of((2, EXT))],
        compiler_params=params(12),
        cost_estimate=cost(2 * ROWS * D * 128, 2 * 1024 * 1024),
    )(mixed, prior, after, taps)


def norm_kernel(
    conv, slope, after, gain, s0, s1, s2, s3, normed, norm_slope, inverse, activated, back, gain_part, centers, squares
):
    spread_sums((s0, s1, s2, s3), (centers, squares))
    center = centers[...]
    inv = lax.rsqrt(squares[...] - center * center + FLOOR)
    norm = (conv[...] - center) * inv
    inverse[...] = inv
    normed[...] = norm
    scale = gain[...]
    scaled = norm * scale
    squash = jax.nn.sigmoid(scaled)
    activated[...] = (scaled * squash)[:ROWS].astype(BF16)
    bend = squash * (1.0 + scaled * (1.0 - squash))
    own = slope[...] * bend[:ROWS]
    gain_part[...] = jnp.sum(own * norm[:ROWS], axis=0, keepdims=True)
    own = own * scale
    past = after[PAD:] * bend[ROWS:] * scale
    norm_slope[:ROWS] = own
    norm_slope[ROWS:] = past
    value = norm_slope[...]
    store_sums(back, value, value * norm)


def norm_of(conv, slope, after, gain, sums):
    ext = shape_of((EXT, W))
    return pl.pallas_call(
        norm_kernel,
        out_shape=[ext, ext, ext, shape_of((ROWS, W), BF16), shape_of((2, EXT)), shape_of((1, W))],
        scratch_shapes=[pltpu.VMEM((EXT, W), F32)] * 2,
        compiler_params=params(16),
        cost_estimate=cost(2 * ROWS * D * 128, 2 * 1024 * 1024),
    )(conv, slope, after, gain, *sums)


def adjoint_kernel(
    normed, norm_slope, inverse, s0, s1, s2, s3, history, taps, sgate, factor, gain_part,
    slopes, taps_part, curve, means, crosses,
):
    spread_sums((s0, s1, s2, s3), (means, crosses))
    curve[...] = inverse[...] * (norm_slope[...] - means[...] - normed[...] * crosses[...])

    @pl.when((lax.axis_index("z") == NZ - 1) & (lax.axis_index("y") == NY - 1))
    def _():
        curve[ROWS:] = jnp.zeros((PAD, W), F32)

    step = 128

    def spread(i, carry):
        base = pl.multiple_of(i * step, step)
        total = swept(curve, taps, base, step, lambda k: k)
        slopes[pl.ds(base, step), :W] = (total * sgate[pl.ds(base, step), :]).astype(BF16)
        slopes[pl.ds(base, step), W:] = (total * factor[pl.ds(base, step), :]).astype(BF16)
        return carry

    lax.fori_loop(0, ROWS // step, spread, 0)

    inner = 64

    def gather(i, sums):
        base = pl.multiple_of(i * inner, inner)
        now = curve[pl.ds(base, inner), :]
        sums = list(sums)
        for residue in range(8):
            ks = [k for k in range(K) if (PAD - k) % 8 == residue]
            low, high = PAD - max(ks), PAD - min(ks)
            block = history[pl.ds(base + low, inner + high - low), :]
            for k in ks:
                at = PAD - k - low
                sums[k] = sums[k] + jnp.sum((now * block[at : at + inner]).reshape(inner // 8, 8, W), axis=0)
        return tuple(sums)

    sums = lax.fori_loop(0, ROWS // inner, gather, tuple(jnp.zeros((8, W), F32) for _ in range(K)))
    for k in range(K):
        taps_part[k : k + 1, :] = jnp.sum(sums[k], axis=0, keepdims=True)
    taps_part[K:, :] = gain_part[...]


def adjoint_of(normed, norm_slope, inverse, back, history, taps, sgate, factor, gain_part):
    return pl.pallas_call(
        adjoint_kernel,
        out_shape=[shape_of((ROWS, 2 * W), BF16), shape_of((K + 1, W))],
        scratch_shapes=[pltpu.VMEM((EXT, W), F32)] * 3,
        compiler_params=params(16),
        cost_estimate=cost(2 * ROWS * D * 256, 2 * 1024 * 1024),
    )(normed, norm_slope, inverse, *back, history, taps, sgate, factor, gain_part)


def across(cols, side):
    return lax.dot_general(cols, side, (((0,), (0,)), ((), ())), preferred_element_type=F32)


def out_grad_kernel(rows, activated, out):
    step = D // NZ
    for z in range(NZ):
        part = across(rows[:, z * step : (z + 1) * step], activated[...]).astype(BF16)
        out[:, z * (D // 32) : (z + 1) * (D // 32), :] = part.reshape(NY, D // 32, W)


def out_grad_of(grad_output, activated):
    return pl.pallas_call(
        out_grad_kernel,
        out_shape=shape_of((NY, D // NY, W), BF16),
        compiler_params=params(8),
        cost_estimate=cost(2 * ROWS * D * 256, 5 * 1024 * 1024),
    )(grad_output, activated)


def weight_grad_kernel(rows, slopes, out_part, taps_part, out):
    small = taps_part[...].astype(BF16)
    block = jnp.concatenate([small[:16], small[16:], jnp.zeros((16, W), BF16)], axis=1)
    for y in range(NY):
        out[y, D // NY :, :] = block
    out[:, : D // NY, 2 * W :] = out_part[...]
    step = D // NZ
    for z in range(NZ):
        part = across(rows[:, z * step : (z + 1) * step], slopes[...]).astype(BF16)
        out[:, z * (D // 32) : (z + 1) * (D // 32), : 2 * W] = part.reshape(NY, D // 32, 2 * W)


def weight_grad_of(block_input, slopes, out_part, taps_part):
    return pl.pallas_call(
        weight_grad_kernel,
        out_shape=shape_of((NY, D // NY + TAIL, 3 * W), BF16),
        compiler_params=params(12),
        cost_estimate=cost(2 * ROWS * D * 256, 7 * 1024 * 1024),
    )(block_input, slopes, out_part, taps_part)


def middle_kernel(arrived, out):
    total = arrived[0].astype(F32)
    for y in range(1, NY):
        total = total + arrived[y].astype(F32)
    total = total.astype(BF16)
    out[:, : D // 32, :] = total[: D // NY].reshape(NZ, D // 32, 3 * W)
    for z in range(NZ):
        out[z, D // 32 :, :] = total[D // NY :]


def middle_of(arrived):
    return pl.pallas_call(
        middle_kernel,
        out_shape=shape_of((NZ, D // 32 + TAIL, 3 * W), BF16),
        compiler_params=params(12),
        cost_estimate=cost(2 * ROWS * D, 2 * 1024 * 1024),
    )(arrived)


def final_kernel(arrived, value_grad, gate_grad, out_grad, taps_grad, gain_grad):
    total = arrived[0].astype(F32)
    for z in range(1, NZ):
        total = total + arrived[z].astype(F32)
    value_grad[...] = total[: D // 32, :W]
    gate_grad[...] = total[: D // 32, W : 2 * W]
    out_grad[...] = total[: D // 32, 2 * W :]
    taps_grad[:16] = total[D // 32 :, :W]
    taps_grad[16:] = total[D // 32 : D // 32 + 15, W : 2 * W]
    gain_grad[...] = total[D // 32 + 15 :, W : 2 * W]


def final_of(arrived):
    part = shape_of((D // 32, W))
    return pl.pallas_call(
        final_kernel,
        out_shape=[part, part, part, shape_of((K, W)), shape_of((1, W))],
        compiler_params=params(12),
        cost_estimate=cost(2 * ROWS * D, 1024 * 1024),
    )(arrived)


def input_grad_kernel(*refs):
    blocks, weights, out = refs[:10], refs[10:18], refs[18]
    half = ROWS // 2
    step = 256
    for r in range(0, ROWS, step):
        total = jnp.zeros((step, D // 8), F32)
        for slot in range(8):
            if slot in (4, 5):
                low, high = blocks[slot], blocks[slot + 4]
                rows = low[r : r + step, :] if r < half else high[r - half : r - half + step, :]
            else:
                rows = blocks[slot][r : r + step, :]
            total = total + lax.dot_general(
                rows, weights[slot][...], (((1,), (1,)), ((), ())), preferred_element_type=F32
            )
        out[r : r + step, :] = total.astype(BF16)


def input_grad_of(blocks, weights):
    return pl.pallas_call(
        input_grad_kernel,
        out_shape=shape_of((ROWS, D // 8), BF16),
        compiler_params=params(16),
        cost_estimate=cost(2 * ROWS * D * 512, 6 * 1024 * 1024),
    )(*blocks, *weights)


def along(value, axis, by):
    count = lax.axis_size(axis)
    return lax.ppermute(value, axis, [(i, (i + by) % count) for i in range(count)])


def from_behind(value, by):
    count = lax.axis_size(SP)
    return lax.ppermute(value, SP, [(i, i + by) for i in range(count) if 0 <= i + by < count])


def to_slot(value, slot):
    pairs = [(t, (t // NC + slot // 2) % NX * NC + (t + slot) % NC) for t in range(NX * NC)]
    return lax.ppermute(value, TP, pairs)


def chip_sums(own):
    pair = own + to_slot(own, 1)
    return [pair, to_slot(pair, 2), to_slot(pair, 6), to_slot(pair, 4)]


def gathered(own):
    half = ROWS // 2
    behind = to_slot(own, 2)
    ahead = to_slot(own, 6)
    other = to_slot(own, 1)
    far_low = to_slot(behind[:half], 2)
    far_high = to_slot(ahead[half:], 6)
    return [own, other, behind, to_slot(behind, 1), far_low, to_slot(far_low, 1), ahead, to_slot(ahead, 1),
            far_high, to_slot(far_high, 1)]


def shards(block_input, value_proj, gate_proj, conv_taps, norm_gain, out_proj, grad_output):
    to_next, to_prior, both, out_side, *cuts = edges(block_input, grad_output, value_proj, gate_proj, out_proj)
    prior = from_behind(to_next, 1)
    after = from_behind(to_prior, -1)
    mixed, sgate, factor = glu(block_input, both)
    history, conv, sums = conv_of(mixed, prior, after, conv_taps)
    sums = chip_sums(sums)
    slope = slopes_of(grad_output, out_side)
    normed, norm_slope, inverse, activated, back, gain_part = norm_of(
        conv, slope, after, norm_gain.reshape(1, W), sums
    )
    back = chip_sums(back)
    out_part = out_grad_of(grad_output, activated)
    slopes, taps_part = adjoint_of(
        normed, norm_slope, inverse, back, history, conv_taps, sgate, factor, gain_part
    )
    partial = weight_grad_of(block_input, slopes, out_part, taps_part)
    partial = lax.all_to_all(partial, "y", 0, 0, tiled=True)
    blocks = gathered(slopes)
    weights = [cuts[0]] + [to_slot(cuts[slot], slot) for slot in range(1, 8)]
    partial = lax.all_to_all(middle_of(partial), "z", 0, 0, tiled=True)
    input_grad = input_grad_of(blocks, weights)
    value_grad, gate_grad, out_grad, taps_grad, gain_grad = final_of(partial)
    return (input_grad, value_grad, gate_grad, out_grad, taps_grad, gain_grad.reshape(W))


def solution(mesh):
    finer = Mesh(mesh.devices.reshape(NZ, NY, NX, NC), ("z", "y", "x", "c"))
    placed = (P(SP, None), P(None, TP), P(None, TP), P(None, TP), P(TP), P(None, TP), P(SP, None))
    split = P(SP, TP)
    return jax.shard_map(
        shards,
        mesh=finer,
        in_specs=placed,
        out_specs=(split, split, split, split, P(None, TP), P(TP)),
        check_vma=False,
    )
```

```python
import jax
import jax.numpy as jnp
from jax import lax
from jax.experimental import pallas as pl
from jax.experimental.pallas import tpu as pltpu
from jax.sharding import Mesh
from jax.sharding import PartitionSpec as P


SP = ("z", "y")
TP = ("x", "c")
NZ, NY, NX, NC = 8, 4, 4, 2
C = 1024
D = 2048
K = 31
ROWS = 1024
W = 128
PAD = 32
EXT = ROWS + PAD
TAIL = 16
BLOCK = D // 8
PART = D // NY
CUT = D // (NY * NZ)
FLOOR = 0.1
F32 = jnp.float32
BF16 = jnp.bfloat16


def params(mib, **more):
    return pltpu.CompilerParams(vmem_limit_bytes=mib * 1024 * 1024, **more)


def cost(flops, size):
    return pl.CostEstimate(flops=flops, bytes_accessed=size, transcendentals=0)


def dot(a, b):
    return jnp.dot(a, b, preferred_element_type=F32)


def shape_of(shape, dtype=F32):
    return jax.ShapeDtypeStruct(shape, dtype)


def edge_kernel(
    rows, grads, value_proj, gate_proj, out_proj, to_next, to_prior, both, out_side, ends, grad_head, sems
):
    pairs = [
        (rows.at[:PAD], ends.at[:PAD]),
        (rows.at[ROWS - PAD :], ends.at[PAD:]),
        (value_proj, both.at[:, :W]),
        (gate_proj, both.at[:, W:]),
        (grads.at[:PAD], grad_head),
        (out_proj, out_side),
    ]
    copies = [pltpu.make_async_copy(a, b, sems.at[i]) for i, (a, b) in enumerate(pairs)]
    for copy in copies:
        copy.start()
    for copy in copies[:4]:
        copy.wait()
    both_parts = dot(ends[...], both[...])
    mixed = (both_parts[:, :W] * jax.nn.sigmoid(both_parts[:, W:])).astype(BF16).astype(F32)
    to_prior[:PAD] = mixed[:PAD]
    to_next[...] = mixed[PAD:]
    for copy in copies[4:]:
        copy.wait()
    to_prior[PAD:] = dot(grad_head[...], out_side[...])


def in_hbm(value):
    return pltpu.with_memory_space_constraint(value, pltpu.HBM)


def edges(block_input, grad_output, value_proj, gate_proj, out_proj):
    hbm = pl.BlockSpec(memory_space=pltpu.HBM)
    vmem = pl.BlockSpec(memory_space=pltpu.VMEM)
    args = [in_hbm(v) for v in (block_input, grad_output, value_proj, gate_proj, out_proj)]
    return pl.pallas_call(
        edge_kernel,
        in_specs=[hbm] * 5,
        out_specs=[vmem] * 4,
        out_shape=[shape_of((PAD, W)), shape_of((2 * PAD, W)), shape_of((D, 2 * W), BF16), shape_of((D, W), BF16)],
        scratch_shapes=[
            pltpu.VMEM((2 * PAD, D), BF16),
            pltpu.VMEM((PAD, D), BF16),
            pltpu.SemaphoreType.DMA((6,)),
        ],
        compiler_params=params(8),
        cost_estimate=cost(2 * 96 * D * 256, 2 * 1024 * 1024),
    )(*args)


def glu_kernel(rows, both, mixed, sgate, factor):
    step = 256
    for r in range(0, ROWS, step):
        parts = dot(rows[r : r + step, :], both[...])
        value = parts[:, :W]
        gate = jax.nn.sigmoid(parts[:, W:])
        mixed[r : r + step, :] = (value * gate).astype(BF16).astype(F32)
        sgate[r : r + step, :] = gate
        factor[r : r + step, :] = value * gate * (1.0 - gate)


def glu(block_input, both):
    return pl.pallas_call(
        glu_kernel,
        out_shape=[shape_of((ROWS, W))] * 3,
        compiler_params=params(12),
        cost_estimate=cost(2 * ROWS * D * 256, 7 * 1024 * 1024),
    )(block_input, both)


def slope_kernel(rows, out_side, both, slope, lend, sems):
    core = lax.axis_index("c")
    copies = []
    for x in range(NX):
        at = pl.multiple_of((x * NC + 1 - core) * BLOCK, BLOCK)
        copies.append(
            pltpu.make_async_copy(
                both.at[pl.ds(at, BLOCK), :], lend.at[x * BLOCK : (x + 1) * BLOCK, :], sems.at[x]
            )
        )
        copies[-1].start()
    slope[...] = dot(rows[...], out_side[...])
    for copy in copies:
        copy.wait()


def slopes_of(grad_output, out_side, both):
    vmem = pl.BlockSpec(memory_space=pltpu.VMEM)
    return pl.pallas_call(
        slope_kernel,
        in_specs=[vmem] * 3,
        out_specs=[vmem] * 2,
        out_shape=[shape_of((ROWS, W)), shape_of((NX * BLOCK, 2 * W), BF16)],
        scratch_shapes=[pltpu.SemaphoreType.DMA((NX,))],
        compiler_params=params(8),
        cost_estimate=cost(2 * ROWS * D * 256, 5 * 1024 * 1024),
    )(grad_output, out_side, both)


def store_sums(out, value, other):
    out[0, :] = jnp.sum(value, axis=1)
    out[1, :] = jnp.sum(other, axis=1)


def spread_sums(parts, outs):
    total = (parts[0][...] + parts[1][...]) + (parts[2][...] + parts[3][...])
    step = 96
    for row, out in enumerate(outs):
        mean = total[row : row + 1, :] * (1.0 / C)
        for r in range(0, EXT, step):
            out[r : r + step, :] = jnp.broadcast_to(mean[:, r : r + step], (W, step)).T


def swept(source, taps, base, step, shifts):
    total = jnp.zeros((step, W), F32)
    for residue in range(8):
        ks = [k for k in range(K) if shifts(k) % 8 == residue]
        low = min(shifts(k) for k in ks)
        high = max(shifts(k) for k in ks)
        block = source[pl.ds(base + low, step + high - low), :]
        for k in ks:
            at = shifts(k) - low
            total = total + taps[k : k + 1, :] * block[at : at + step]
    return total


def conv_kernel(mixed, prior, after, taps, history, conv, sums):
    history[:PAD] = prior[...]
    history[PAD : PAD + ROWS] = mixed[...]
    history[PAD + ROWS :] = after[:PAD]
    step = 96

    def body(i, carry):
        base = pl.multiple_of(i * step, step)
        conv[pl.ds(base, step), :] = swept(history, taps, base, step, lambda k: PAD - k)
        return carry

    lax.fori_loop(0, EXT // step, body, 0)
    value = conv[...]
    store_sums(sums, value, value * value)


def conv_of(mixed, prior, after, taps):
    return pl.pallas_call(
        conv_kernel,
        out_shape=[shape_of((EXT + PAD, W)), shape_of((EXT, W)), shape_of((2, EXT))],
        compiler_params=params(12),
        cost_estimate=cost(2 * ROWS * D * 128, 2 * 1024 * 1024),
    )(mixed, prior, after, taps)


def norm_kernel(
    conv, slope, after, gain, s0, s1, s2, s3, normed, norm_slope, inverse, activated, back, gain_part, centers, squares
):
    spread_sums((s0, s1, s2, s3), (centers, squares))
    center = centers[...]
    inv = lax.rsqrt(squares[...] - center * center + FLOOR)
    norm = (conv[...] - center) * inv
    inverse[...] = inv
    normed[...] = norm
    scale = gain[...]
    scaled = norm * scale
    squash = jax.nn.sigmoid(scaled)
    activated[...] = (scaled * squash)[:ROWS].astype(BF16)
    bend = squash * (1.0 + scaled * (1.0 - squash))
    own = slope[...] * bend[:ROWS]
    gain_part[...] = jnp.sum(own * norm[:ROWS], axis=0, keepdims=True)
    own = own * scale
    past = after[PAD:] * bend[ROWS:] * scale
    norm_slope[:ROWS] = own
    norm_slope[ROWS:] = past
    value = norm_slope[...]
    store_sums(back, value, value * norm)


def norm_of(conv, slope, after, gain, sums):
    ext = shape_of((EXT, W))
    return pl.pallas_call(
        norm_kernel,
        out_shape=[ext, ext, ext, shape_of((ROWS, W), BF16), shape_of((2, EXT)), shape_of((1, W))],
        scratch_shapes=[pltpu.VMEM((EXT, W), F32)] * 2,
        compiler_params=params(16),
        cost_estimate=cost(2 * ROWS * D * 128, 2 * 1024 * 1024),
    )(conv, slope, after, gain, *sums)


def adjoint_kernel(
    normed, norm_slope, inverse, s0, s1, s2, s3, history, taps, sgate, factor, gain_part,
    slopes, taps_part, curve, means, crosses,
):
    spread_sums((s0, s1, s2, s3), (means, crosses))
    curve[...] = inverse[...] * (norm_slope[...] - means[...] - normed[...] * crosses[...])

    @pl.when((lax.axis_index("z") == NZ - 1) & (lax.axis_index("y") == NY - 1))
    def _():
        curve[ROWS:] = jnp.zeros((PAD, W), F32)

    step = 128

    def spread(i, carry):
        base = pl.multiple_of(i * step, step)
        total = swept(curve, taps, base, step, lambda k: k)
        slopes[pl.ds(base, step), :W] = (total * sgate[pl.ds(base, step), :]).astype(BF16)
        slopes[pl.ds(base, step), W:] = (total * factor[pl.ds(base, step), :]).astype(BF16)
        return carry

    lax.fori_loop(0, ROWS // step, spread, 0)

    inner = 64

    def gather(i, sums):
        base = pl.multiple_of(i * inner, inner)
        now = curve[pl.ds(base, inner), :]
        sums = list(sums)
        for residue in range(8):
            ks = [k for k in range(K) if (PAD - k) % 8 == residue]
            low, high = PAD - max(ks), PAD - min(ks)
            block = history[pl.ds(base + low, inner + high - low), :]
            for k in ks:
                at = PAD - k - low
                sums[k] = sums[k] + jnp.sum((now * block[at : at + inner]).reshape(inner // 8, 8, W), axis=0)
        return tuple(sums)

    sums = lax.fori_loop(0, ROWS // inner, gather, tuple(jnp.zeros((8, W), F32) for _ in range(K)))
    for k in range(K):
        taps_part[k : k + 1, :] = jnp.sum(sums[k], axis=0, keepdims=True)
    taps_part[K:, :] = gain_part[...]


def adjoint_of(normed, norm_slope, inverse, back, history, taps, sgate, factor, gain_part):
    return pl.pallas_call(
        adjoint_kernel,
        out_shape=[shape_of((ROWS, 2 * W), BF16), shape_of((K + 1, W))],
        scratch_shapes=[pltpu.VMEM((EXT, W), F32)] * 3,
        compiler_params=params(16),
        cost_estimate=cost(2 * ROWS * D * 256, 2 * 1024 * 1024),
    )(normed, norm_slope, inverse, *back, history, taps, sgate, factor, gain_part)


def across(rows, side, parts):
    step = D // NZ
    for z in range(NZ):
        part = lax.dot_general(
            rows[:, z * step : (z + 1) * step], side, (((0,), (0,)), ((), ())), preferred_element_type=F32
        )
        parts[:, z * CUT : (z + 1) * CUT, :] = part.astype(BF16).reshape(NY, CUT, side.shape[1])


def out_grad_kernel(rows, activated, *rest):
    outs, parts = rest[:NY], rest[NY]
    across(rows, activated[...], parts)
    for by, out in enumerate(outs):
        out[...] = parts[lax.rem(lax.axis_index("y") + by, NY)]


def out_grad_of(grad_output, activated):
    return pl.pallas_call(
        out_grad_kernel,
        out_shape=[shape_of((PART, W), BF16)] * NY,
        scratch_shapes=[pltpu.VMEM((NY, PART, W), BF16)],
        compiler_params=params(8),
        cost_estimate=cost(2 * ROWS * D * 256, 5 * 1024 * 1024),
    )(grad_output, activated)


def weight_grad_kernel(rows, slopes, taps_part, *rest):
    outs, parts = rest[:NY], rest[NY]
    across(rows, slopes[...], parts)
    small = taps_part[...].astype(BF16)
    small = jnp.concatenate([small[:TAIL], small[TAIL:]], axis=1)
    for by, out in enumerate(outs):
        out[:PART] = parts[lax.rem(lax.axis_index("y") + by, NY)]
        out[PART:] = small


def weight_grad_of(block_input, slopes, taps_part):
    return pl.pallas_call(
        weight_grad_kernel,
        out_shape=[shape_of((PART + TAIL, 2 * W), BF16)] * NY,
        scratch_shapes=[pltpu.VMEM((NY, PART, 2 * W), BF16)],
        compiler_params=params(12),
        cost_estimate=cost(2 * ROWS * D * 256, 7 * 1024 * 1024),
    )(block_input, slopes, taps_part)


def summed(parts):
    total = parts[0][...].astype(F32)
    for part in parts[1:]:
        total = total + part[...].astype(F32)
    return total


def middle_kernel(*refs):
    both, outs, out = refs[:NY], refs[NY : 2 * NY], refs[2 * NY]
    total = summed(both).astype(BF16)
    out[:, :CUT, : 2 * W] = total[:PART].reshape(NZ, CUT, 2 * W)
    out[:, :CUT, 2 * W :] = summed(outs).astype(BF16).reshape(NZ, CUT, W)
    tail = jnp.concatenate([total[PART:], jnp.zeros((TAIL, W), BF16)], axis=1)
    for z in range(NZ):
        out[z, CUT:, :] = tail


def middle_of(both, outs):
    return pl.pallas_call(
        middle_kernel,
        out_shape=shape_of((NZ, CUT + TAIL, 3 * W), BF16),
        compiler_params=params(12),
        cost_estimate=cost(2 * ROWS * D, 2 * 1024 * 1024),
    )(*both, *outs)


def final_kernel(arrived, value_grad, gate_grad, out_grad, taps_grad, gain_grad):
    total = arrived[0].astype(F32)
    for z in range(1, NZ):
        total = total + arrived[z].astype(F32)
    value_grad[...] = total[: CUT, :W]
    gate_grad[...] = total[: CUT, W : 2 * W]
    out_grad[...] = total[: CUT, 2 * W :]
    taps_grad[:16] = total[CUT :, :W]
    taps_grad[16:] = total[CUT : CUT + 15, W : 2 * W]
    gain_grad[...] = total[CUT + 15 :, W : 2 * W]


def final_of(arrived):
    part = shape_of((CUT, W))
    return pl.pallas_call(
        final_kernel,
        out_shape=[part, part, part, shape_of((K, W)), shape_of((1, W))],
        compiler_params=params(12),
        cost_estimate=cost(2 * ROWS * D, 1024 * 1024),
    )(arrived)


def share(by, slopes, others, both, lent):
    here = lax.axis_index("x")
    core = lax.axis_index("c")
    chip = lax.rem(here + by * (1 - 2 * core) + NX, NX)
    mine = both[pl.ds(pl.multiple_of((chip * NC + core) * BLOCK, BLOCK), BLOCK), :]
    theirs = lent[pl.ds(pl.multiple_of(chip * BLOCK, BLOCK), BLOCK), :]
    contract = (((1,), (1,)), ((), ()))
    total = lax.dot_general(slopes[...], mine, contract, preferred_element_type=F32)
    return total + lax.dot_general(others[...], theirs, contract, preferred_element_type=F32)


def far_kernel(slopes, others, both, lent, far, back):
    far[...] = share(2, slopes, others, both, lent).astype(BF16)
    back[...] = share(-1, slopes, others, both, lent).astype(BF16)


def near_kernel(slopes, others, both, lent, arrived, near):
    near[...] = (share(1, slopes, others, both, lent) + arrived[...].astype(F32)).astype(BF16)


def own_kernel(slopes, others, both, lent, first, second, out):
    total = share(0, slopes, others, both, lent)
    out[...] = (total + first[...].astype(F32) + second[...].astype(F32)).astype(BF16)


def share_call(kernel, count, shares, *args):
    piece = shape_of((ROWS, BLOCK), BF16)
    return pl.pallas_call(
        kernel,
        out_shape=[piece] * count,
        compiler_params=params(12),
        cost_estimate=cost(2 * ROWS * D * 256 * shares, shares * 2 * 1024 * 1024),
    )(*args)


def from_behind(value, by):
    count = lax.axis_size(SP)
    return lax.ppermute(value, SP, [(i, i + by) for i in range(count) if 0 <= i + by < count])


def to_slot(value, slot):
    pairs = [(t, (t // NC + slot // 2) % NX * NC + (t + slot) % NC) for t in range(NX * NC)]
    return lax.ppermute(value, TP, pairs)


def chip_sums(own):
    pair = own + to_slot(own, 1)
    return [pair, to_slot(pair, 2), to_slot(pair, 6), to_slot(pair, 4)]


def along(value, by):
    pairs = [(t, (t // NC + (by if t % NC == 0 else -by)) % NX * NC + t % NC) for t in range(NX * NC)]
    return lax.ppermute(value, TP, pairs)


def spread_y(parts):
    return [parts[0]] + [
        lax.ppermute(parts[by], "y", [(y, (y + by) % NY) for y in range(NY)]) for by in (1, 3, 2)
    ]


def shards(block_input, value_proj, gate_proj, conv_taps, norm_gain, out_proj, grad_output):
    to_next, to_prior, both, out_side = edges(block_input, grad_output, value_proj, gate_proj, out_proj)
    prior = from_behind(to_next, 1)
    after = from_behind(to_prior, -1)
    mixed, sgate, factor = glu(block_input, both)
    history, conv, sums = conv_of(mixed, prior, after, conv_taps)
    sums = chip_sums(sums)
    slope, lend = slopes_of(grad_output, out_side, both)
    normed, norm_slope, inverse, activated, back, gain_part = norm_of(
        conv, slope, after, norm_gain.reshape(1, W), sums
    )
    back = chip_sums(back)
    out_parts = out_grad_of(grad_output, activated)
    out_parts = spread_y(out_parts)
    slopes, taps_part = adjoint_of(
        normed, norm_slope, inverse, back, history, conv_taps, sgate, factor, gain_part
    )
    others = to_slot(slopes, 1)
    both_parts = weight_grad_of(block_input, slopes, taps_part)
    both_parts = spread_y(both_parts)
    lent = to_slot(lend, 1)
    sides = (slopes, others, both, lent)
    far, single = share_call(far_kernel, 2, 2, *sides)
    arrived = along(far, 1)
    (near,) = share_call(near_kernel, 1, 1, *sides, arrived)
    near = along(near, 1)
    single = along(single, -1)
    partial = middle_of(both_parts, out_parts)
    partial = lax.all_to_all(partial, "z", 0, 0, tiled=True)
    (input_grad,) = share_call(own_kernel, 1, 1, *sides, near, single)
    value_grad, gate_grad, out_grad, taps_grad, gain_grad = final_of(partial)
    return (input_grad, value_grad, gate_grad, out_grad, taps_grad, gain_grad.reshape(W))


def solution(mesh):
    finer = Mesh(mesh.devices.reshape(NZ, NY, NX, NC), ("z", "y", "x", "c"))
    placed = (P(SP, None), P(None, TP), P(None, TP), P(None, TP), P(TP), P(None, TP), P(SP, None))
    split = P(SP, TP)
    return jax.shard_map(
        shards,
        mesh=finer,
        in_specs=placed,
        out_specs=(split, split, split, split, P(None, TP), P(TP)),
        check_vma=False,
    )
```

```python
import jax
import jax.numpy as jnp
from jax import lax
from jax.experimental import pallas as pl
from jax.experimental.pallas import tpu as pltpu
from jax.sharding import Mesh
from jax.sharding import PartitionSpec as P


SP = ("z", "y")
TP = ("x", "c")
NZ, NY, NX, NC = 8, 4, 4, 2
C = 1024
D = 2048
K = 31
ROWS = 1024
W = 128
PAD = 32
EXT = ROWS + PAD
TAIL = 16
BLOCK = D // 8
PART = D // NY
CUT = D // (NY * NZ)
FLOOR = 0.1
F32 = jnp.float32
BF16 = jnp.bfloat16


def params(mib, **more):
    return pltpu.CompilerParams(vmem_limit_bytes=mib * 1024 * 1024, **more)


def cost(flops, size):
    return pl.CostEstimate(flops=flops, bytes_accessed=size, transcendentals=0)


def dot(a, b):
    return jnp.dot(a, b, preferred_element_type=F32)


def shape_of(shape, dtype=F32):
    return jax.ShapeDtypeStruct(shape, dtype)


def edge_kernel(
    rows, grads, value_proj, gate_proj, out_proj, to_next, to_prior, both, out_side, ends, grad_head, sems
):
    pairs = [
        (rows.at[:PAD], ends.at[:PAD]),
        (rows.at[ROWS - PAD :], ends.at[PAD:]),
        (value_proj, both.at[:, :W]),
        (gate_proj, both.at[:, W:]),
        (grads.at[:PAD], grad_head),
        (out_proj, out_side),
    ]
    copies = [pltpu.make_async_copy(a, b, sems.at[i]) for i, (a, b) in enumerate(pairs)]
    for copy in copies:
        copy.start()
    for copy in copies[:4]:
        copy.wait()
    both_parts = dot(ends[...], both[...])
    mixed = (both_parts[:, :W] * jax.nn.sigmoid(both_parts[:, W:])).astype(BF16).astype(F32)
    to_prior[:PAD] = mixed[:PAD]
    to_next[...] = mixed[PAD:]
    for copy in copies[4:]:
        copy.wait()
    to_prior[PAD:] = dot(grad_head[...], out_side[...])


def in_hbm(value):
    return pltpu.with_memory_space_constraint(value, pltpu.HBM)


def edges(block_input, grad_output, value_proj, gate_proj, out_proj):
    hbm = pl.BlockSpec(memory_space=pltpu.HBM)
    vmem = pl.BlockSpec(memory_space=pltpu.VMEM)
    args = [in_hbm(v) for v in (block_input, grad_output, value_proj, gate_proj, out_proj)]
    return pl.pallas_call(
        edge_kernel,
        in_specs=[hbm] * 5,
        out_specs=[vmem] * 4,
        out_shape=[shape_of((PAD, W)), shape_of((2 * PAD, W)), shape_of((D, 2 * W), BF16), shape_of((D, W), BF16)],
        scratch_shapes=[
            pltpu.VMEM((2 * PAD, D), BF16),
            pltpu.VMEM((PAD, D), BF16),
            pltpu.SemaphoreType.DMA((6,)),
        ],
        compiler_params=params(8),
        cost_estimate=cost(2 * 96 * D * 256, 2 * 1024 * 1024),
    )(*args)


def glu_kernel(rows, both, mixed, sgate, factor):
    step = 256
    for r in range(0, ROWS, step):
        parts = dot(rows[r : r + step, :], both[...])
        value = parts[:, :W]
        gate = jax.nn.sigmoid(parts[:, W:])
        mixed[r : r + step, :] = (value * gate).astype(BF16).astype(F32)
        sgate[r : r + step, :] = gate
        factor[r : r + step, :] = value * gate * (1.0 - gate)


def glu(block_input, both):
    return pl.pallas_call(
        glu_kernel,
        out_shape=[shape_of((ROWS, W))] * 3,
        compiler_params=params(12),
        cost_estimate=cost(2 * ROWS * D * 256, 7 * 1024 * 1024),
    )(block_input, both)


def slope_kernel(rows, out_side, both, slope, lend, sems):
    core = lax.axis_index("c")
    copies = []
    for x in range(NX):
        at = pl.multiple_of((x * NC + 1 - core) * BLOCK, BLOCK)
        copies.append(
            pltpu.make_async_copy(
                both.at[pl.ds(at, BLOCK), :], lend.at[x * BLOCK : (x + 1) * BLOCK, :], sems.at[x]
            )
        )
        copies[-1].start()
    slope[...] = dot(rows[...], out_side[...])
    for copy in copies:
        copy.wait()


def slopes_of(grad_output, out_side, both):
    vmem = pl.BlockSpec(memory_space=pltpu.VMEM)
    return pl.pallas_call(
        slope_kernel,
        in_specs=[vmem] * 3,
        out_specs=[vmem] * 2,
        out_shape=[shape_of((ROWS, W)), shape_of((NX * BLOCK, 2 * W), BF16)],
        scratch_shapes=[pltpu.SemaphoreType.DMA((NX,))],
        compiler_params=params(8),
        cost_estimate=cost(2 * ROWS * D * 256, 5 * 1024 * 1024),
    )(grad_output, out_side, both)


def store_sums(out, value, other):
    out[0, :] = jnp.sum(value, axis=1)
    out[1, :] = jnp.sum(other, axis=1)


def spread_sums(parts, outs):
    total = (parts[0][...] + parts[1][...]) + (parts[2][...] + parts[3][...])
    step = 96
    for row, out in enumerate(outs):
        mean = total[row : row + 1, :] * (1.0 / C)
        for r in range(0, EXT, step):
            out[r : r + step, :] = jnp.broadcast_to(mean[:, r : r + step], (W, step)).T


def swept(source, taps, base, step, shifts):
    total = jnp.zeros((step, W), F32)
    for residue in range(8):
        ks = [k for k in range(K) if shifts(k) % 8 == residue]
        low = min(shifts(k) for k in ks)
        high = max(shifts(k) for k in ks)
        block = source[pl.ds(base + low, step + high - low), :]
        for k in ks:
            at = shifts(k) - low
            total = total + taps[k : k + 1, :] * block[at : at + step]
    return total


def conv_kernel(mixed, prior, after, taps, history, conv, sums):
    history[:PAD] = prior[...]
    history[PAD : PAD + ROWS] = mixed[...]
    history[PAD + ROWS :] = after[:PAD]
    step = 96

    def body(i, carry):
        base = pl.multiple_of(i * step, step)
        conv[pl.ds(base, step), :] = swept(history, taps, base, step, lambda k: PAD - k)
        return carry

    lax.fori_loop(0, EXT // step, body, 0)
    value = conv[...]
    store_sums(sums, value, value * value)


def conv_of(mixed, prior, after, taps):
    return pl.pallas_call(
        conv_kernel,
        out_shape=[shape_of((EXT + PAD, W)), shape_of((EXT, W)), shape_of((2, EXT))],
        compiler_params=params(12),
        cost_estimate=cost(2 * ROWS * D * 128, 2 * 1024 * 1024),
    )(mixed, prior, after, taps)


def norm_kernel(
    conv, slope, after, gain, s0, s1, s2, s3, normed, norm_slope, inverse, activated, back, gain_part, centers, squares
):
    spread_sums((s0, s1, s2, s3), (centers, squares))
    center = centers[...]
    inv = lax.rsqrt(squares[...] - center * center + FLOOR)
    norm = (conv[...] - center) * inv
    inverse[...] = inv
    normed[...] = norm
    scale = gain[...]
    scaled = norm * scale
    squash = jax.nn.sigmoid(scaled)
    activated[...] = (scaled * squash)[:ROWS].astype(BF16)
    bend = squash * (1.0 + scaled * (1.0 - squash))
    own = slope[...] * bend[:ROWS]
    gain_part[...] = jnp.sum(own * norm[:ROWS], axis=0, keepdims=True)
    own = own * scale
    past = after[PAD:] * bend[ROWS:] * scale
    norm_slope[:ROWS] = own
    norm_slope[ROWS:] = past
    value = norm_slope[...]
    store_sums(back, value, value * norm)


def norm_of(conv, slope, after, gain, sums):
    ext = shape_of((EXT, W))
    return pl.pallas_call(
        norm_kernel,
        out_shape=[ext, ext, ext, shape_of((ROWS, W), BF16), shape_of((2, EXT)), shape_of((1, W))],
        scratch_shapes=[pltpu.VMEM((EXT, W), F32)] * 2,
        compiler_params=params(16),
        cost_estimate=cost(2 * ROWS * D * 128, 2 * 1024 * 1024),
    )(conv, slope, after, gain, *sums)


def adjoint_kernel(
    normed, norm_slope, inverse, s0, s1, s2, s3, history, taps, sgate, factor, gain_part,
    slopes, taps_part, curve, means, crosses,
):
    spread_sums((s0, s1, s2, s3), (means, crosses))
    curve[...] = inverse[...] * (norm_slope[...] - means[...] - normed[...] * crosses[...])

    @pl.when((lax.axis_index("z") == NZ - 1) & (lax.axis_index("y") == NY - 1))
    def _():
        curve[ROWS:] = jnp.zeros((PAD, W), F32)

    step = 128

    def spread(i, carry):
        base = pl.multiple_of(i * step, step)
        total = swept(curve, taps, base, step, lambda k: k)
        slopes[pl.ds(base, step), :W] = (total * sgate[pl.ds(base, step), :]).astype(BF16)
        slopes[pl.ds(base, step), W:] = (total * factor[pl.ds(base, step), :]).astype(BF16)
        return carry

    lax.fori_loop(0, ROWS // step, spread, 0)

    inner = 64

    def gather(i, sums):
        base = pl.multiple_of(i * inner, inner)
        now = curve[pl.ds(base, inner), :]
        sums = list(sums)
        for residue in range(8):
            ks = [k for k in range(K) if (PAD - k) % 8 == residue]
            low, high = PAD - max(ks), PAD - min(ks)
            block = history[pl.ds(base + low, inner + high - low), :]
            for k in ks:
                at = PAD - k - low
                sums[k] = sums[k] + jnp.sum((now * block[at : at + inner]).reshape(inner // 8, 8, W), axis=0)
        return tuple(sums)

    sums = lax.fori_loop(0, ROWS // inner, gather, tuple(jnp.zeros((8, W), F32) for _ in range(K)))
    for k in range(K):
        taps_part[k : k + 1, :] = jnp.sum(sums[k], axis=0, keepdims=True)
    taps_part[K:, :] = gain_part[...]


def adjoint_of(normed, norm_slope, inverse, back, history, taps, sgate, factor, gain_part):
    return pl.pallas_call(
        adjoint_kernel,
        out_shape=[shape_of((ROWS, 2 * W), BF16), shape_of((K + 1, W))],
        scratch_shapes=[pltpu.VMEM((EXT, W), F32)] * 3,
        compiler_params=params(16),
        cost_estimate=cost(2 * ROWS * D * 256, 2 * 1024 * 1024),
    )(normed, norm_slope, inverse, *back, history, taps, sgate, factor, gain_part)


def across(rows, side, parts):
    step = D // NZ
    for z in range(NZ):
        part = lax.dot_general(
            rows[:, z * step : (z + 1) * step], side, (((0,), (0,)), ((), ())), preferred_element_type=F32
        )
        parts[:, z * CUT : (z + 1) * CUT, :] = part.astype(BF16).reshape(NY, CUT, side.shape[1])


def out_grad_kernel(rows, activated, *rest):
    outs, parts = rest[:NY], rest[NY]
    across(rows, activated[...], parts)
    for by, out in enumerate(outs):
        out[...] = parts[lax.rem(lax.axis_index("y") + by, NY)]


def out_grad_of(grad_output, activated):
    return pl.pallas_call(
        out_grad_kernel,
        out_shape=[shape_of((PART, W), BF16)] * NY,
        scratch_shapes=[pltpu.VMEM((NY, PART, W), BF16)],
        compiler_params=params(8),
        cost_estimate=cost(2 * ROWS * D * 256, 5 * 1024 * 1024),
    )(grad_output, activated)


def weight_grad_kernel(rows, slopes, taps_part, *rest):
    outs, parts = rest[:NY], rest[NY]
    across(rows, slopes[...], parts)
    small = taps_part[...].astype(BF16)
    small = jnp.concatenate([small[:TAIL], small[TAIL:]], axis=1)
    for by, out in enumerate(outs):
        out[:PART] = parts[lax.rem(lax.axis_index("y") + by, NY)]
        out[PART:] = small


def weight_grad_of(block_input, slopes, taps_part):
    return pl.pallas_call(
        weight_grad_kernel,
        out_shape=[shape_of((PART + TAIL, 2 * W), BF16)] * NY,
        scratch_shapes=[pltpu.VMEM((NY, PART, 2 * W), BF16)],
        compiler_params=params(12),
        cost_estimate=cost(2 * ROWS * D * 256, 7 * 1024 * 1024),
    )(block_input, slopes, taps_part)


def summed(parts):
    total = parts[0][...].astype(F32)
    for part in parts[1:]:
        total = total + part[...].astype(F32)
    return total


def middle_kernel(*refs):
    both, side, outs, parts = refs[:NY], refs[NY : 2 * NY], refs[2 * NY : 2 * NY + NZ], refs[2 * NY + NZ]
    total = summed(both).astype(BF16)
    parts[:, :CUT, :] = total[:PART, :W].reshape(NZ, CUT, W)
    parts[:, CUT : 2 * CUT, :] = total[:PART, W:].reshape(NZ, CUT, W)
    parts[:, 2 * CUT :, :] = summed(side).astype(BF16).reshape(NZ, CUT, W)
    for by, out in enumerate(outs):
        out[: 3 * CUT] = parts[lax.rem(lax.axis_index("z") + by, NZ)]
        out[3 * CUT : 3 * CUT + TAIL] = total[PART:, :W]
        out[3 * CUT + TAIL :] = total[PART:, W:]


def middle_of(both, side):
    return pl.pallas_call(
        middle_kernel,
        out_shape=[shape_of((3 * CUT + 2 * TAIL, W), BF16)] * NZ,
        scratch_shapes=[pltpu.VMEM((NZ, 3 * CUT, W), BF16)],
        compiler_params=params(12),
        cost_estimate=cost(2 * ROWS * D, 2 * 1024 * 1024),
    )(*both, *side)


def final_kernel(*refs):
    parts, (value_grad, gate_grad, out_grad, taps_grad, gain_grad) = refs[:NZ], refs[NZ:]
    total = summed(parts)
    value_grad[...] = total[:CUT]
    gate_grad[...] = total[CUT : 2 * CUT]
    out_grad[...] = total[2 * CUT : 3 * CUT]
    taps_grad[...] = total[3 * CUT : 3 * CUT + K]
    gain_grad[...] = total[3 * CUT + K :]


def final_of(parts):
    part = shape_of((CUT, W))
    return pl.pallas_call(
        final_kernel,
        out_shape=[part, part, part, shape_of((K, W)), shape_of((1, W))],
        compiler_params=params(12),
        cost_estimate=cost(2 * ROWS * D, 1024 * 1024),
    )(*parts)


def share(by, slopes, others, both, lent):
    here = lax.axis_index("x")
    core = lax.axis_index("c")
    chip = lax.rem(here + by * (1 - 2 * core) + NX, NX)
    mine = both[pl.ds(pl.multiple_of((chip * NC + core) * BLOCK, BLOCK), BLOCK), :]
    theirs = lent[pl.ds(pl.multiple_of(chip * BLOCK, BLOCK), BLOCK), :]
    contract = (((1,), (1,)), ((), ()))
    total = lax.dot_general(slopes[...], mine, contract, preferred_element_type=F32)
    return total + lax.dot_general(others[...], theirs, contract, preferred_element_type=F32)


def far_kernel(slopes, others, both, lent, far, back):
    far[...] = share(2, slopes, others, both, lent).astype(BF16)
    back[...] = share(-1, slopes, others, both, lent).astype(BF16)


def near_kernel(slopes, others, both, lent, arrived, near):
    near[...] = (share(1, slopes, others, both, lent) + arrived[...].astype(F32)).astype(BF16)


def own_kernel(slopes, others, both, lent, first, second, out):
    total = share(0, slopes, others, both, lent)
    out[...] = (total + first[...].astype(F32) + second[...].astype(F32)).astype(BF16)


def share_call(kernel, count, shares, *args):
    piece = shape_of((ROWS, BLOCK), BF16)
    return pl.pallas_call(
        kernel,
        out_shape=[piece] * count,
        compiler_params=params(12),
        cost_estimate=cost(2 * ROWS * D * 256 * shares, shares * 2 * 1024 * 1024),
    )(*args)


def from_behind(value, by):
    count = lax.axis_size(SP)
    return lax.ppermute(value, SP, [(i, i + by) for i in range(count) if 0 <= i + by < count])


def to_slot(value, slot):
    pairs = [(t, (t // NC + slot // 2) % NX * NC + (t + slot) % NC) for t in range(NX * NC)]
    return lax.ppermute(value, TP, pairs)


def chip_sums(own):
    pair = own + to_slot(own, 1)
    return [pair, to_slot(pair, 2), to_slot(pair, 6), to_slot(pair, 4)]


def along(value, by):
    pairs = [(t, (t // NC + (by if t % NC == 0 else -by)) % NX * NC + t % NC) for t in range(NX * NC)]
    return lax.ppermute(value, TP, pairs)


def further(value, axis, by):
    count = lax.axis_size(axis)
    return lax.ppermute(value, axis, [(i, (i + by) % count) for i in range(count)])


def spread(parts, axis, order):
    return [parts[0]] + [further(parts[by], axis, by) for by in order]


def shards(block_input, value_proj, gate_proj, conv_taps, norm_gain, out_proj, grad_output):
    to_next, to_prior, both, out_side = edges(block_input, grad_output, value_proj, gate_proj, out_proj)
    prior = from_behind(to_next, 1)
    after = from_behind(to_prior, -1)
    mixed, sgate, factor = glu(block_input, both)
    history, conv, sums = conv_of(mixed, prior, after, conv_taps)
    sums = chip_sums(sums)
    slope, lend = slopes_of(grad_output, out_side, both)
    normed, norm_slope, inverse, activated, back, gain_part = norm_of(
        conv, slope, after, norm_gain.reshape(1, W), sums
    )
    back = chip_sums(back)
    out_parts = out_grad_of(grad_output, activated)
    out_parts = spread(out_parts, "y", Y_ORDER)
    slopes, taps_part = adjoint_of(normed, norm_slope, inverse, back, history, conv_taps, sgate, factor, gain_part)
    others = to_slot(slopes, 1)
    both_parts = weight_grad_of(block_input, slopes, taps_part)
    both_parts = spread(both_parts, "y", Y_ORDER)
    lent = to_slot(lend, 1)
    sides = (slopes, others, both, lent)
    far, single = share_call(far_kernel, 2, 2, *sides)
    arrived = along(far, 1)
    (near,) = share_call(near_kernel, 1, 1, *sides, arrived)
    near = along(near, 1)
    single = along(single, -1)
    parts = middle_of(both_parts, out_parts)
    parts = spread(parts, "z", Z_ORDER)
    (input_grad,) = share_call(own_kernel, 1, 1, *sides, near, single)
    value_grad, gate_grad, out_grad, taps_grad, gain_grad = final_of(parts)
    return (input_grad, value_grad, gate_grad, out_grad, taps_grad, gain_grad.reshape(W))


Y_ORDER = (2, 1, 3)
Z_ORDER = (4, 3, 5, 2, 6, 1, 7)


def solution(mesh):
    finer = Mesh(mesh.devices.reshape(NZ, NY, NX, NC), ("z", "y", "x", "c"))
    placed = (P(SP, None), P(None, TP), P(None, TP), P(None, TP), P(TP), P(None, TP), P(SP, None))
    split = P(SP, TP)
    return jax.shard_map(
        shards,
        mesh=finer,
        in_specs=placed,
        out_specs=(split, split, split, split, P(None, TP), P(TP)),
        check_vma=False,
    )
```

```python
import jax
import jax.numpy as jnp
from jax import lax
from jax.experimental import pallas as pl
from jax.experimental.pallas import tpu as pltpu
from jax.sharding import Mesh
from jax.sharding import PartitionSpec as P


SP = ("z", "y")
TP = ("x", "c")
NZ, NY, NX, NC = 8, 4, 4, 2
C = 1024
D = 2048
K = 31
ROWS = 1024
W = 128
PAD = 32
EXT = ROWS + PAD
TAIL = 16
BLOCK = D // 8
SLOTS = NZ // NC
PART = D // (NY * NC)
CUT = D // (NY * NZ)
PIECE = 3 * CUT + 2 * TAIL
FLOOR = 0.1
F32 = jnp.float32
BF16 = jnp.bfloat16


def params(mib, **more):
    return pltpu.CompilerParams(vmem_limit_bytes=mib * 1024 * 1024, **more)


def cost(flops, size):
    return pl.CostEstimate(flops=flops, bytes_accessed=size, transcendentals=0)


def dot(a, b):
    return jnp.dot(a, b, preferred_element_type=F32)


def shape_of(shape, dtype=F32):
    return jax.ShapeDtypeStruct(shape, dtype)


def edge_kernel(
    rows, grads, value_proj, gate_proj, out_proj, to_next, to_prior, both, out_side, ends, grad_head, sems
):
    pairs = [
        (rows.at[:PAD], ends.at[:PAD]),
        (rows.at[ROWS - PAD :], ends.at[PAD:]),
        (value_proj, both.at[:, :W]),
        (gate_proj, both.at[:, W:]),
        (grads.at[:PAD], grad_head),
        (out_proj, out_side),
    ]
    copies = [pltpu.make_async_copy(a, b, sems.at[i]) for i, (a, b) in enumerate(pairs)]
    for copy in copies:
        copy.start()
    for copy in copies[:4]:
        copy.wait()
    both_parts = dot(ends[...], both[...])
    mixed = (both_parts[:, :W] * jax.nn.sigmoid(both_parts[:, W:])).astype(BF16).astype(F32)
    to_prior[:PAD] = mixed[:PAD]
    to_next[...] = mixed[PAD:]
    for copy in copies[4:]:
        copy.wait()
    to_prior[PAD:] = dot(grad_head[...], out_side[...])


def in_hbm(value):
    return pltpu.with_memory_space_constraint(value, pltpu.HBM)


def edges(block_input, grad_output, value_proj, gate_proj, out_proj):
    hbm = pl.BlockSpec(memory_space=pltpu.HBM)
    vmem = pl.BlockSpec(memory_space=pltpu.VMEM)
    args = [in_hbm(v) for v in (block_input, grad_output, value_proj, gate_proj, out_proj)]
    return pl.pallas_call(
        edge_kernel,
        in_specs=[hbm] * 5,
        out_specs=[vmem] * 4,
        out_shape=[shape_of((PAD, W)), shape_of((2 * PAD, W)), shape_of((D, 2 * W), BF16), shape_of((D, W), BF16)],
        scratch_shapes=[
            pltpu.VMEM((2 * PAD, D), BF16),
            pltpu.VMEM((PAD, D), BF16),
            pltpu.SemaphoreType.DMA((6,)),
        ],
        compiler_params=params(8),
        cost_estimate=cost(2 * 96 * D * 256, 2 * 1024 * 1024),
    )(*args)


def glu_kernel(rows, both, mixed, sgate, factor):
    step = 256
    for r in range(0, ROWS, step):
        parts = dot(rows[r : r + step, :], both[...])
        value = parts[:, :W]
        gate = jax.nn.sigmoid(parts[:, W:])
        mixed[r : r + step, :] = (value * gate).astype(BF16).astype(F32)
        sgate[r : r + step, :] = gate
        factor[r : r + step, :] = value * gate * (1.0 - gate)


def glu(block_input, both):
    return pl.pallas_call(
        glu_kernel,
        out_shape=[shape_of((ROWS, W))] * 3,
        compiler_params=params(12),
        cost_estimate=cost(2 * ROWS * D * 256, 7 * 1024 * 1024),
    )(block_input, both)


def slope_kernel(rows, out_side, both, slope, lend, sems):
    core = lax.axis_index("c")
    copies = []
    for x in range(NX):
        at = pl.multiple_of((x * NC + 1 - core) * BLOCK, BLOCK)
        copies.append(
            pltpu.make_async_copy(
                both.at[pl.ds(at, BLOCK), :], lend.at[x * BLOCK : (x + 1) * BLOCK, :], sems.at[x]
            )
        )
        copies[-1].start()
    slope[...] = dot(rows[...], out_side[...])
    for copy in copies:
        copy.wait()


def slopes_of(grad_output, out_side, both):
    vmem = pl.BlockSpec(memory_space=pltpu.VMEM)
    return pl.pallas_call(
        slope_kernel,
        in_specs=[vmem] * 3,
        out_specs=[vmem] * 2,
        out_shape=[shape_of((ROWS, W)), shape_of((NX * BLOCK, 2 * W), BF16)],
        scratch_shapes=[pltpu.SemaphoreType.DMA((NX,))],
        compiler_params=params(8),
        cost_estimate=cost(2 * ROWS * D * 256, 5 * 1024 * 1024),
    )(grad_output, out_side, both)


def store_sums(out, value, other):
    out[0, :] = jnp.sum(value, axis=1)
    out[1, :] = jnp.sum(other, axis=1)


def spread_sums(parts, outs):
    total = (parts[0][...] + parts[1][...]) + (parts[2][...] + parts[3][...])
    step = 96
    for row, out in enumerate(outs):
        mean = total[row : row + 1, :] * (1.0 / C)
        for r in range(0, EXT, step):
            out[r : r + step, :] = jnp.broadcast_to(mean[:, r : r + step], (W, step)).T


def swept(source, taps, base, step, shifts):
    total = jnp.zeros((step, W), F32)
    for residue in range(8):
        ks = [k for k in range(K) if shifts(k) % 8 == residue]
        low = min(shifts(k) for k in ks)
        high = max(shifts(k) for k in ks)
        block = source[pl.ds(base + low, step + high - low), :]
        for k in ks:
            at = shifts(k) - low
            total = total + taps[k : k + 1, :] * block[at : at + step]
    return total


def conv_kernel(mixed, taps, conv, sums, history):
    history[:PAD] = jnp.zeros((PAD, W), F32)
    history[PAD:] = mixed[...]
    step = 128

    def body(i, carry):
        base = pl.multiple_of(i * step, step)
        conv[pl.ds(base, step), :] = swept(history, taps, base, step, lambda k: PAD - k)
        return carry

    lax.fori_loop(0, ROWS // step, body, 0)
    value = conv[...]
    store_sums(sums, value, value * value)


def conv_of(mixed, taps):
    return pl.pallas_call(
        conv_kernel,
        out_shape=[shape_of((ROWS, W)), shape_of((2, ROWS))],
        scratch_shapes=[pltpu.VMEM((PAD + ROWS, W), F32)],
        compiler_params=params(12),
        cost_estimate=cost(2 * ROWS * D * 128, 2 * 1024 * 1024),
    )(mixed, taps)


def edge_conv_kernel(mixed, prior, after, taps, main_sums, edge, sums, low, high):
    low[:PAD] = prior[...]
    low[PAD:] = mixed[:PAD]
    high[:PAD] = mixed[ROWS - PAD :]
    high[PAD:] = after[:PAD]
    edge[:PAD] = swept(low, taps, 0, PAD, lambda k: PAD - k)
    edge[PAD:] = swept(high, taps, 0, PAD, lambda k: PAD - k)
    value = edge[...]
    sums[:, PAD:ROWS] = main_sums[:, PAD:]
    for row, term in enumerate((value, value * value)):
        ends = jnp.sum(term, axis=1)[None]
        sums[row : row + 1, :PAD] = ends[:, :PAD]
        sums[row : row + 1, ROWS:] = ends[:, PAD:]


def edge_conv_of(mixed, prior, after, taps, main_sums):
    return pl.pallas_call(
        edge_conv_kernel,
        out_shape=[shape_of((2 * PAD, W)), shape_of((2, EXT))],
        scratch_shapes=[pltpu.VMEM((2 * PAD, W), F32)] * 2,
        compiler_params=params(8),
        cost_estimate=cost(2 * ROWS * D * 16, 1024 * 1024),
    )(mixed, prior, after, taps, main_sums)


def norm_kernel(
    main, edge, slope, after, gain, s0, s1, s2, s3, normed, norm_slope, inverse, activated, back, gain_part,
    centers, squares,
):
    normed[:PAD] = edge[:PAD]
    normed[PAD:ROWS] = main[PAD:]
    normed[ROWS:] = edge[PAD:]
    spread_sums((s0, s1, s2, s3), (centers, squares))
    center = centers[...]
    inv = lax.rsqrt(squares[...] - center * center + FLOOR)
    norm = (normed[...] - center) * inv
    inverse[...] = inv
    normed[...] = norm
    scale = gain[...]
    scaled = norm * scale
    squash = jax.nn.sigmoid(scaled)
    activated[...] = (scaled * squash)[:ROWS].astype(BF16)
    bend = squash * (1.0 + scaled * (1.0 - squash))
    own = slope[...] * bend[:ROWS]
    gain_part[...] = jnp.sum(own * norm[:ROWS], axis=0, keepdims=True)
    own = own * scale
    past = after[PAD:] * bend[ROWS:] * scale
    norm_slope[:ROWS] = own
    norm_slope[ROWS:] = past
    value = norm_slope[...]
    store_sums(back, value, value * norm)


def norm_of(main, edge, slope, after, gain, sums):
    ext = shape_of((EXT, W))
    return pl.pallas_call(
        norm_kernel,
        out_shape=[ext, ext, ext, shape_of((ROWS, W), BF16), shape_of((2, EXT)), shape_of((1, W))],
        scratch_shapes=[pltpu.VMEM((EXT, W), F32)] * 2,
        compiler_params=params(16),
        cost_estimate=cost(2 * ROWS * D * 128, 2 * 1024 * 1024),
    )(main, edge, slope, after, gain, *sums)


def adjoint_kernel(
    normed, norm_slope, inverse, s0, s1, s2, s3, mixed, prior, taps, sgate, factor, gain_part,
    slopes, curve, means, crosses, history, taps_part,
):
    history[:PAD] = prior[...]
    history[PAD:] = mixed[...]
    spread_sums((s0, s1, s2, s3), (means, crosses))
    curve[...] = inverse[...] * (norm_slope[...] - means[...] - normed[...] * crosses[...])

    @pl.when((lax.axis_index("z") == NZ - 1) & (lax.axis_index("y") == NY - 1))
    def _():
        curve[ROWS:] = jnp.zeros((PAD, W), F32)

    step = 128

    def spread(i, carry):
        base = pl.multiple_of(i * step, step)
        total = swept(curve, taps, base, step, lambda k: k)
        slopes[pl.ds(base, step), :W] = (total * sgate[pl.ds(base, step), :]).astype(BF16)
        slopes[pl.ds(base, step), W:] = (total * factor[pl.ds(base, step), :]).astype(BF16)
        return carry

    lax.fori_loop(0, ROWS // step, spread, 0)

    inner = 64

    def gather(i, sums):
        base = pl.multiple_of(i * inner, inner)
        now = curve[pl.ds(base, inner), :]
        sums = list(sums)
        for residue in range(8):
            ks = [k for k in range(K) if (PAD - k) % 8 == residue]
            low, high = PAD - max(ks), PAD - min(ks)
            block = history[pl.ds(base + low, inner + high - low), :]
            for k in ks:
                at = PAD - k - low
                sums[k] = sums[k] + jnp.sum((now * block[at : at + inner]).reshape(inner // 8, 8, W), axis=0)
        return tuple(sums)

    sums = lax.fori_loop(0, ROWS // inner, gather, tuple(jnp.zeros((8, W), F32) for _ in range(K)))
    for k in range(K):
        taps_part[k : k + 1, :] = jnp.sum(sums[k], axis=0, keepdims=True)
    taps_part[K:, :] = gain_part[...]
    small = taps_part[...].astype(BF16)
    slopes[ROWS:, :W] = small[:TAIL]
    slopes[ROWS:, W:] = small[TAIL:]


def adjoint_of(normed, norm_slope, inverse, back, mixed, prior, taps, sgate, factor, gain_part):
    return pl.pallas_call(
        adjoint_kernel,
        out_shape=shape_of((ROWS + TAIL, 2 * W), BF16),
        scratch_shapes=[pltpu.VMEM((EXT, W), F32)] * 4 + [pltpu.VMEM((K + 1, W), F32)],
        compiler_params=params(16),
        cost_estimate=cost(2 * ROWS * D * 256, 2 * 1024 * 1024),
    )(normed, norm_slope, inverse, *back, mixed, prior, taps, sgate, factor, gain_part)


def kept_by(slot):
    core = lax.axis_index("c")
    by = 4 * (1 - core) if slot == 0 else slot * (1 - 2 * core) + NZ
    return lax.rem(lax.axis_index("z") + by, NZ)


def across(rows, side, parts, lanes):
    step = D // NZ
    for slot in range(SLOTS):
        at = pl.multiple_of(kept_by(slot) * step, step)
        part = lax.dot_general(
            rows[:, pl.ds(at, step)], side, (((0,), (0,)), ((), ())), preferred_element_type=F32
        )
        parts[:, slot * CUT : (slot + 1) * CUT, lanes] = part.astype(BF16).reshape(NY, CUT, side.shape[1])


def along_y(by):
    return lax.rem(lax.axis_index("y") + by, NY)


def out_grad_kernel(rows, activated, other, *rest):
    outs, parts = rest[:NY], rest[NY]
    across(rows, activated[...], parts, slice(0, W))
    across(rows, other[...], parts, slice(W, 2 * W))
    for by, out in enumerate(outs):
        out[...] = parts[along_y(by)]


def out_grad_of(grad_output, activated, other):
    return pl.pallas_call(
        out_grad_kernel,
        out_shape=[shape_of((PART, 2 * W), BF16)] * NY,
        scratch_shapes=[pltpu.VMEM((NY, PART, 2 * W), BF16)],
        compiler_params=params(8),
        cost_estimate=cost(2 * ROWS * D * 256, 5 * 1024 * 1024),
    )(grad_output, activated, other)


def own_weight_grad_kernel(rows, slopes, parts):
    across(rows, slopes[:ROWS], parts, slice(0, 2 * W))


def own_weight_grad_of(block_input, slopes):
    return pl.pallas_call(
        own_weight_grad_kernel,
        out_shape=shape_of((NY, PART, 2 * W), BF16),
        compiler_params=params(8),
        cost_estimate=cost(2 * ROWS * D * 128, 3 * 1024 * 1024),
    )(block_input, slopes)


def weight_grad_kernel(rows, slopes, others, own, *rest):
    outs, parts = rest[:NY], rest[NY]
    across(rows, others[:ROWS], parts, slice(0, 2 * W))
    for by, out in enumerate(outs):
        out[:PART, : 2 * W] = own[along_y(by)]
        out[:PART, 2 * W :] = parts[along_y(by)]
        out[PART:, : 2 * W] = slopes[ROWS:]
        out[PART:, 2 * W :] = others[ROWS:]


def weight_grad_of(block_input, slopes, others, own):
    return pl.pallas_call(
        weight_grad_kernel,
        out_shape=[shape_of((PART + TAIL, 4 * W), BF16)] * NY,
        scratch_shapes=[pltpu.VMEM((NY, PART, 2 * W), BF16)],
        compiler_params=params(12),
        cost_estimate=cost(2 * ROWS * D * 128, 5 * 1024 * 1024),
    )(block_input, slopes, others, own)


def summed(parts):
    total = parts[0][...].astype(F32)
    for part in parts[1:]:
        total = total + part[...].astype(F32)
    return total


def middle_kernel(*refs):
    both, side, outs = refs[:NY], refs[NY : 2 * NY], refs[2 * NY :]
    total = summed(both).astype(BF16)
    outer = summed(side).astype(BF16)
    for slot, out in enumerate(outs):
        rows = slice(slot * CUT, (slot + 1) * CUT)
        for core in range(NC):
            at, lane = core * PIECE, core * 2 * W
            out[at : at + CUT] = total[rows, lane : lane + W]
            out[at + CUT : at + 2 * CUT] = total[rows, lane + W : lane + 2 * W]
            out[at + 2 * CUT : at + 3 * CUT] = outer[rows, core * W : (core + 1) * W]
            out[at + 3 * CUT : at + 3 * CUT + TAIL] = total[PART:, lane : lane + W]
            out[at + 3 * CUT + TAIL : at + PIECE] = total[PART:, lane + W : lane + 2 * W]


def middle_of(both, side):
    return pl.pallas_call(
        middle_kernel,
        out_shape=[shape_of((NC * PIECE, W), BF16)] * SLOTS,
        compiler_params=params(12),
        cost_estimate=cost(2 * ROWS * D, 2 * 1024 * 1024),
    )(*both, *side)


def chip_kernel(mine, opposite, one, two, three, own, other):
    first = jnp.where(lax.axis_index("c") == 0, opposite[...].astype(F32), mine[...].astype(F32))
    total = first + summed((one, two, three))
    own[...] = total[:PIECE]
    other[...] = total[PIECE:]


def chip_of(mine, parts):
    return pl.pallas_call(
        chip_kernel,
        out_shape=[shape_of((PIECE, W))] * 2,
        compiler_params=params(8),
        cost_estimate=cost(2 * ROWS * D, 1024 * 1024),
    )(mine, *parts)


def final_kernel(own, other, value_grad, gate_grad, out_grad, taps_grad, gain_grad):
    total = own[...] + other[...]
    value_grad[...] = total[:CUT]
    gate_grad[...] = total[CUT : 2 * CUT]
    out_grad[...] = total[2 * CUT : 3 * CUT]
    taps_grad[...] = total[3 * CUT : 3 * CUT + K]
    gain_grad[...] = total[3 * CUT + K :]


def final_of(own, other):
    part = shape_of((CUT, W))
    return pl.pallas_call(
        final_kernel,
        out_shape=[part, part, part, shape_of((K, W)), shape_of((1, W))],
        compiler_params=params(8),
        cost_estimate=cost(2 * ROWS * D, 1024 * 1024),
    )(own, other)


def share(by, slopes, others, both, lent):
    here = lax.axis_index("x")
    core = lax.axis_index("c")
    chip = lax.rem(here + by * (1 - 2 * core) + NX, NX)
    mine = both[pl.ds(pl.multiple_of((chip * NC + core) * BLOCK, BLOCK), BLOCK), :]
    theirs = lent[pl.ds(pl.multiple_of(chip * BLOCK, BLOCK), BLOCK), :]
    contract = (((1,), (1,)), ((), ()))
    total = lax.dot_general(slopes[:ROWS], mine, contract, preferred_element_type=F32)
    return total + lax.dot_general(others[:ROWS], theirs, contract, preferred_element_type=F32)


def far_kernel(slopes, others, both, lent, far, back):
    far[...] = share(2, slopes, others, both, lent).astype(BF16)
    back[...] = share(-1, slopes, others, both, lent).astype(BF16)


def near_kernel(slopes, others, both, lent, arrived, near):
    near[...] = (share(1, slopes, others, both, lent) + arrived[...].astype(F32)).astype(BF16)


def own_kernel(slopes, others, both, lent, first, second, out):
    total = share(0, slopes, others, both, lent)
    out[...] = (total + first[...].astype(F32) + second[...].astype(F32)).astype(BF16)


def share_call(kernel, count, shares, *args):
    piece = shape_of((ROWS, BLOCK), BF16)
    return pl.pallas_call(
        kernel,
        out_shape=[piece] * count,
        compiler_params=params(12),
        cost_estimate=cost(2 * ROWS * D * 256 * shares, shares * 2 * 1024 * 1024),
    )(*args)


def from_behind(value, by):
    count = lax.axis_size(SP)
    return lax.ppermute(value, SP, [(i, i + by) for i in range(count) if 0 <= i + by < count])


def to_slot(value, slot):
    pairs = [(t, (t // NC + slot // 2) % NX * NC + (t + slot) % NC) for t in range(NX * NC)]
    return lax.ppermute(value, TP, pairs)


def chip_sums(own):
    pair = own + to_slot(own, 1)
    return [pair] + [to_slot(pair, slot) for slot in (2, 6, 4)]


def along(value, by):
    pairs = [(t, (t // NC + (by if t % NC == 0 else -by)) % NX * NC + t % NC) for t in range(NX * NC)]
    return lax.ppermute(value, TP, pairs)


def further(value, axis, by):
    count = lax.axis_size(axis)
    return lax.ppermute(value, axis, [(i, (i + by) % count) for i in range(count)])


def spread(parts, axis, order):
    return [parts[0]] + [further(parts[by], axis, by) for by in order]


def to_keeper(value, slot):
    if slot == 0:
        pairs = [(z * NC, (z + 4) % NZ * NC) for z in range(NZ)]
    else:
        pairs = [
            (z * NC + c, (z + (slot if c == 0 else -slot)) % NZ * NC + c) for z in range(NZ) for c in range(NC)
        ]
    return lax.ppermute(value, ("z", "c"), pairs)


def shards(block_input, value_proj, gate_proj, conv_taps, norm_gain, out_proj, grad_output):
    to_next, to_prior, both, out_side = edges(block_input, grad_output, value_proj, gate_proj, out_proj)
    prior = from_behind(to_next, 1)
    after = from_behind(to_prior, -1)
    mixed, sgate, factor = glu(block_input, both)
    conv, sums = conv_of(mixed, conv_taps)
    edge, sums = edge_conv_of(mixed, prior, after, conv_taps, sums)
    sums = chip_sums(sums)
    slope, lend = slopes_of(grad_output, out_side, both)
    normed, norm_slope, inverse, activated, back, gain_part = norm_of(
        conv, edge, slope, after, norm_gain.reshape(1, W), sums
    )
    back = chip_sums(back)
    other_activated = to_slot(activated, 1)
    out_parts = out_grad_of(grad_output, activated, other_activated)
    out_parts = spread(out_parts, "y", Y_ORDER)
    slopes = adjoint_of(
        normed, norm_slope, inverse, back, mixed, prior, conv_taps, sgate, factor, gain_part
    )
    others = to_slot(slopes, 1)
    own_parts = own_weight_grad_of(block_input, slopes)
    both_parts = weight_grad_of(block_input, slopes, others, own_parts)
    both_parts = spread(both_parts, "y", Y_ORDER)
    lent = to_slot(lend, 1)
    sides = (slopes, others, both, lent)
    far, single = share_call(far_kernel, 2, 2, *sides)
    arrived = along(far, 1)
    (near,) = share_call(near_kernel, 1, 1, *sides, arrived)
    near = along(near, 1)
    single = along(single, -1)
    parts = middle_of(both_parts, out_parts)
    sent = {slot: to_keeper(parts[slot], slot) for slot in Z_ORDER}
    own, other = chip_of(parts[0], [sent[slot] for slot in range(SLOTS)])
    other = to_slot(other, 1)
    (input_grad,) = share_call(own_kernel, 1, 1, *sides, near, single)
    value_grad, gate_grad, out_grad, taps_grad, gain_grad = final_of(own, other)
    return (input_grad, value_grad, gate_grad, out_grad, taps_grad, gain_grad.reshape(W))


Y_ORDER = (2, 1, 3)
Z_ORDER = (0, 3, 2, 1)


def solution(mesh):
    finer = Mesh(mesh.devices.reshape(NZ, NY, NX, NC), ("z", "y", "x", "c"))
    placed = (P(SP, None), P(None, TP), P(None, TP), P(None, TP), P(TP), P(None, TP), P(SP, None))
    split = P(SP, TP)
    return jax.shard_map(
        shards,
        mesh=finer,
        in_specs=placed,
        out_specs=(split, split, split, split, P(None, TP), P(TP)),
        check_vma=False,
    )
```

```python
import jax
import jax.numpy as jnp
from jax import lax
from jax.experimental import pallas as pl
from jax.experimental.pallas import tpu as pltpu
from jax.sharding import Mesh
from jax.sharding import PartitionSpec as P


SP = ("z", "y")
TP = ("x", "c")
NZ, NY, NX, NC = 8, 4, 4, 2
C = 1024
D = 2048
K = 31
ROWS = 1024
W = 128
PAD = 32
EXT = ROWS + PAD
BLOCK = D // 8
SLOTS = NZ // NC
PART = D // (NY * NC)
CUT = D // (NY * NZ)
PIECE = 3 * CUT + K + 1
FLOOR = 0.1
F32 = jnp.float32
BF16 = jnp.bfloat16


def params(mib, **more):
    return pltpu.CompilerParams(vmem_limit_bytes=mib * 1024 * 1024, **more)


def cost(flops, size):
    return pl.CostEstimate(flops=flops, bytes_accessed=size, transcendentals=0)


def dot(a, b):
    return jnp.dot(a, b, preferred_element_type=F32)


def shape_of(shape, dtype=F32):
    return jax.ShapeDtypeStruct(shape, dtype)


def edge_kernel(
    rows, grads, value_proj, gate_proj, out_proj, to_next, to_prior, both, out_side, ends, grad_head, sems
):
    pairs = [
        (rows.at[:PAD], ends.at[:PAD]),
        (rows.at[ROWS - PAD :], ends.at[PAD:]),
        (value_proj, both.at[:, :W]),
        (gate_proj, both.at[:, W:]),
        (grads.at[:PAD], grad_head),
        (out_proj, out_side),
    ]
    copies = [pltpu.make_async_copy(a, b, sems.at[i]) for i, (a, b) in enumerate(pairs)]
    for copy in copies:
        copy.start()
    for copy in copies[:4]:
        copy.wait()
    both_parts = dot(ends[...], both[...])
    mixed = (both_parts[:, :W] * jax.nn.sigmoid(both_parts[:, W:])).astype(BF16).astype(F32)
    to_prior[:PAD] = mixed[:PAD]
    to_next[...] = mixed[PAD:]
    for copy in copies[4:]:
        copy.wait()
    to_prior[PAD:] = dot(grad_head[...], out_side[...])


def in_hbm(value):
    return pltpu.with_memory_space_constraint(value, pltpu.HBM)


def edges(block_input, grad_output, value_proj, gate_proj, out_proj):
    hbm = pl.BlockSpec(memory_space=pltpu.HBM)
    vmem = pl.BlockSpec(memory_space=pltpu.VMEM)
    args = [in_hbm(v) for v in (block_input, grad_output, value_proj, gate_proj, out_proj)]
    return pl.pallas_call(
        edge_kernel,
        in_specs=[hbm] * 5,
        out_specs=[vmem] * 4,
        out_shape=[shape_of((PAD, W)), shape_of((2 * PAD, W)), shape_of((D, 2 * W), BF16), shape_of((D, W), BF16)],
        scratch_shapes=[
            pltpu.VMEM((2 * PAD, D), BF16),
            pltpu.VMEM((PAD, D), BF16),
            pltpu.SemaphoreType.DMA((6,)),
        ],
        compiler_params=params(8),
        cost_estimate=cost(2 * 96 * D * 256, 2 * 1024 * 1024),
    )(*args)


def glu_kernel(rows, both, mixed, sgate, factor):
    step = 256
    for r in range(0, ROWS, step):
        parts = dot(rows[r : r + step, :], both[...])
        value = parts[:, :W]
        gate = jax.nn.sigmoid(parts[:, W:])
        mixed[r : r + step, :] = (value * gate).astype(BF16).astype(F32)
        sgate[r : r + step, :] = gate
        factor[r : r + step, :] = value * gate * (1.0 - gate)


def glu(block_input, both):
    return pl.pallas_call(
        glu_kernel,
        out_shape=[shape_of((ROWS, W))] * 3,
        compiler_params=params(12),
        cost_estimate=cost(2 * ROWS * D * 256, 7 * 1024 * 1024),
    )(block_input, both)


def slope_kernel(rows, out_side, both, slope, lend, sems):
    core = lax.axis_index("c")
    copies = []
    for x in range(NX):
        at = pl.multiple_of((x * NC + 1 - core) * BLOCK, BLOCK)
        copies.append(
            pltpu.make_async_copy(
                both.at[pl.ds(at, BLOCK), :], lend.at[x * BLOCK : (x + 1) * BLOCK, :], sems.at[x]
            )
        )
        copies[-1].start()
    slope[...] = dot(rows[...], out_side[...])
    for copy in copies:
        copy.wait()


def slopes_of(grad_output, out_side, both):
    vmem = pl.BlockSpec(memory_space=pltpu.VMEM)
    return pl.pallas_call(
        slope_kernel,
        in_specs=[vmem] * 3,
        out_specs=[vmem] * 2,
        out_shape=[shape_of((ROWS, W)), shape_of((NX * BLOCK, 2 * W), BF16)],
        scratch_shapes=[pltpu.SemaphoreType.DMA((NX,))],
        compiler_params=params(8),
        cost_estimate=cost(2 * ROWS * D * 256, 5 * 1024 * 1024),
    )(grad_output, out_side, both)


def store_sums(out, value, other):
    out[0, :] = jnp.sum(value, axis=1)
    out[1, :] = jnp.sum(other, axis=1)


def spread_sums(parts, outs):
    total = (parts[0][...] + parts[1][...]) + (parts[2][...] + parts[3][...])
    step = 96
    for row, out in enumerate(outs):
        mean = total[row : row + 1, :] * (1.0 / C)
        for r in range(0, EXT, step):
            out[r : r + step, :] = jnp.broadcast_to(mean[:, r : r + step], (W, step)).T


def swept(source, taps, base, step, shifts):
    total = jnp.zeros((step, W), F32)
    for residue in range(8):
        ks = [k for k in range(K) if shifts(k) % 8 == residue]
        low = min(shifts(k) for k in ks)
        high = max(shifts(k) for k in ks)
        block = source[pl.ds(base + low, step + high - low), :]
        for k in ks:
            at = shifts(k) - low
            total = total + taps[k : k + 1, :] * block[at : at + step]
    return total


def conv_kernel(mixed, taps, conv, sums, history):
    history[:PAD] = jnp.zeros((PAD, W), F32)
    history[PAD:] = mixed[...]
    step = 128

    def body(i, carry):
        base = pl.multiple_of(i * step, step)
        conv[pl.ds(base, step), :] = swept(history, taps, base, step, lambda k: PAD - k)
        return carry

    lax.fori_loop(0, ROWS // step, body, 0)
    value = conv[...]
    store_sums(sums, value, value * value)


def conv_of(mixed, taps):
    return pl.pallas_call(
        conv_kernel,
        out_shape=[shape_of((ROWS, W)), shape_of((2, ROWS))],
        scratch_shapes=[pltpu.VMEM((PAD + ROWS, W), F32)],
        compiler_params=params(12),
        cost_estimate=cost(2 * ROWS * D * 128, 2 * 1024 * 1024),
    )(mixed, taps)


def edge_conv_kernel(mixed, prior, after, taps, main_sums, edge, sums, low, high):
    low[:PAD] = prior[...]
    low[PAD:] = mixed[:PAD]
    high[:PAD] = mixed[ROWS - PAD :]
    high[PAD:] = after[:PAD]
    edge[:PAD] = swept(low, taps, 0, PAD, lambda k: PAD - k)
    edge[PAD:] = swept(high, taps, 0, PAD, lambda k: PAD - k)
    value = edge[...]
    sums[:, PAD:ROWS] = main_sums[:, PAD:]
    for row, term in enumerate((value, value * value)):
        ends = jnp.sum(term, axis=1)[None]
        sums[row : row + 1, :PAD] = ends[:, :PAD]
        sums[row : row + 1, ROWS:] = ends[:, PAD:]


def edge_conv_of(mixed, prior, after, taps, main_sums):
    return pl.pallas_call(
        edge_conv_kernel,
        out_shape=[shape_of((2 * PAD, W)), shape_of((2, EXT))],
        scratch_shapes=[pltpu.VMEM((2 * PAD, W), F32)] * 2,
        compiler_params=params(8),
        cost_estimate=cost(2 * ROWS * D * 16, 1024 * 1024),
    )(mixed, prior, after, taps, main_sums)


def norm_kernel(
    main, edge, slope, after, gain, s0, s1, s2, s3, normed, norm_slope, inverse, activated, back, gain_part,
    centers, squares,
):
    normed[:PAD] = edge[:PAD]
    normed[PAD:ROWS] = main[PAD:]
    normed[ROWS:] = edge[PAD:]
    spread_sums((s0, s1, s2, s3), (centers, squares))
    center = centers[...]
    inv = lax.rsqrt(squares[...] - center * center + FLOOR)
    norm = (normed[...] - center) * inv
    inverse[...] = inv
    normed[...] = norm
    scale = gain[...]
    scaled = norm * scale
    squash = jax.nn.sigmoid(scaled)
    activated[...] = (scaled * squash)[:ROWS].astype(BF16)
    bend = squash * (1.0 + scaled * (1.0 - squash))
    own = slope[...] * bend[:ROWS]
    gain_part[...] = jnp.sum(own * norm[:ROWS], axis=0, keepdims=True)
    own = own * scale
    past = after[PAD:] * bend[ROWS:] * scale
    norm_slope[:ROWS] = own
    norm_slope[ROWS:] = past
    value = norm_slope[...]
    store_sums(back, value, value * norm)


def norm_of(main, edge, slope, after, gain, sums):
    ext = shape_of((EXT, W))
    return pl.pallas_call(
        norm_kernel,
        out_shape=[ext, ext, ext, shape_of((ROWS, W), BF16), shape_of((2, EXT)), shape_of((1, W))],
        scratch_shapes=[pltpu.VMEM((EXT, W), F32)] * 2,
        compiler_params=params(16),
        cost_estimate=cost(2 * ROWS * D * 128, 2 * 1024 * 1024),
    )(main, edge, slope, after, gain, *sums)


def adjoint_kernel(
    normed, norm_slope, inverse, s0, s1, s2, s3, taps, sgate, factor, slopes, curve, means, crosses
):
    spread_sums((s0, s1, s2, s3), (means, crosses))
    curve[...] = inverse[...] * (norm_slope[...] - means[...] - normed[...] * crosses[...])

    @pl.when((lax.axis_index("z") == NZ - 1) & (lax.axis_index("y") == NY - 1))
    def _():
        curve[ROWS:] = jnp.zeros((PAD, W), F32)

    step = 128

    def spread(i, carry):
        base = pl.multiple_of(i * step, step)
        total = swept(curve, taps, base, step, lambda k: k)
        slopes[pl.ds(base, step), :W] = (total * sgate[pl.ds(base, step), :]).astype(BF16)
        slopes[pl.ds(base, step), W:] = (total * factor[pl.ds(base, step), :]).astype(BF16)
        return carry

    lax.fori_loop(0, ROWS // step, spread, 0)


def adjoint_of(normed, norm_slope, inverse, back, taps, sgate, factor):
    return pl.pallas_call(
        adjoint_kernel,
        out_shape=[shape_of((ROWS, 2 * W), BF16), shape_of((EXT, W))],
        scratch_shapes=[pltpu.VMEM((EXT, W), F32)] * 2,
        compiler_params=params(16),
        cost_estimate=cost(2 * ROWS * D * 256, 2 * 1024 * 1024),
    )(normed, norm_slope, inverse, *back, taps, sgate, factor)


def taps_kernel(curve, mixed, prior, gain_part, taps_part, history):
    history[:PAD] = prior[...]
    history[PAD:] = mixed[...]
    inner = 64

    def gather(i, sums):
        base = pl.multiple_of(i * inner, inner)
        now = curve[pl.ds(base, inner), :]
        sums = list(sums)
        for residue in range(8):
            ks = [k for k in range(K) if (PAD - k) % 8 == residue]
            low, high = PAD - max(ks), PAD - min(ks)
            block = history[pl.ds(base + low, inner + high - low), :]
            for k in ks:
                at = PAD - k - low
                sums[k] = sums[k] + jnp.sum((now * block[at : at + inner]).reshape(inner // 8, 8, W), axis=0)
        return tuple(sums)

    sums = lax.fori_loop(0, ROWS // inner, gather, tuple(jnp.zeros((8, W), F32) for _ in range(K)))
    for k in range(K):
        taps_part[k : k + 1, :] = jnp.sum(sums[k], axis=0, keepdims=True)
    taps_part[K:, :] = gain_part[...]


def taps_of(curve, mixed, prior, gain_part):
    return pl.pallas_call(
        taps_kernel,
        out_shape=shape_of((K + 1, W)),
        scratch_shapes=[pltpu.VMEM((PAD + ROWS, W), F32)],
        compiler_params=params(8),
        cost_estimate=cost(2 * ROWS * D * 64, 1024 * 1024),
    )(curve, mixed, prior, gain_part)


def kept_by(slot):
    core = lax.axis_index("c")
    by = 4 * (1 - core) if slot == 0 else slot * (1 - 2 * core) + NZ
    return lax.rem(lax.axis_index("z") + by, NZ)


def across(rows, side, parts, lanes):
    step = D // NZ
    for slot in range(SLOTS):
        at = pl.multiple_of(kept_by(slot) * step, step)
        part = lax.dot_general(
            rows[:, pl.ds(at, step)], side, (((0,), (0,)), ((), ())), preferred_element_type=F32
        )
        parts[:, slot * CUT : (slot + 1) * CUT, lanes] = part.astype(BF16).reshape(NY, CUT, side.shape[1])


def along_y(by):
    return lax.rem(lax.axis_index("y") + by, NY)


def out_grad_kernel(rows, activated, other, *rest):
    outs, parts = rest[:NY], rest[NY]
    across(rows, activated[...], parts, slice(0, W))
    across(rows, other[...], parts, slice(W, 2 * W))
    for by, out in enumerate(outs):
        out[...] = parts[along_y(by)]


def out_grad_of(grad_output, activated, other):
    return pl.pallas_call(
        out_grad_kernel,
        out_shape=[shape_of((PART, 2 * W), BF16)] * NY,
        scratch_shapes=[pltpu.VMEM((NY, PART, 2 * W), BF16)],
        compiler_params=params(8),
        cost_estimate=cost(2 * ROWS * D * 256, 5 * 1024 * 1024),
    )(grad_output, activated, other)


def own_weight_grad_kernel(rows, slopes, parts):
    across(rows, slopes[...], parts, slice(0, 2 * W))


def own_weight_grad_of(block_input, slopes):
    return pl.pallas_call(
        own_weight_grad_kernel,
        out_shape=shape_of((NY, PART, 2 * W), BF16),
        compiler_params=params(8),
        cost_estimate=cost(2 * ROWS * D * 128, 3 * 1024 * 1024),
    )(block_input, slopes)


def weight_grad_kernel(rows, others, own, *rest):
    outs, parts = rest[:NY], rest[NY]
    across(rows, others[...], parts, slice(0, 2 * W))
    for by, out in enumerate(outs):
        out[:, : 2 * W] = own[along_y(by)]
        out[:, 2 * W :] = parts[along_y(by)]


def weight_grad_of(block_input, others, own):
    return pl.pallas_call(
        weight_grad_kernel,
        out_shape=[shape_of((PART, 4 * W), BF16)] * NY,
        scratch_shapes=[pltpu.VMEM((NY, PART, 2 * W), BF16)],
        compiler_params=params(12),
        cost_estimate=cost(2 * ROWS * D * 128, 5 * 1024 * 1024),
    )(block_input, others, own)


def summed(parts):
    total = parts[0][...].astype(F32)
    for part in parts[1:]:
        total = total + part[...].astype(F32)
    return total


def middle_kernel(*refs):
    both, side, small, outs = refs[:NY], refs[NY : 2 * NY], refs[2 * NY : 3 * NY], refs[3 * NY :]
    total = summed(both).astype(BF16)
    outer = summed(side).astype(BF16)
    tail = summed(small).astype(BF16)
    for slot, out in enumerate(outs):
        rows = slice(slot * CUT, (slot + 1) * CUT)
        for core in range(NC):
            at, lane = core * PIECE, core * 2 * W
            out[at : at + CUT] = total[rows, lane : lane + W]
            out[at + CUT : at + 2 * CUT] = total[rows, lane + W : lane + 2 * W]
            out[at + 2 * CUT : at + 3 * CUT] = outer[rows, core * W : (core + 1) * W]
            out[at + 3 * CUT : at + PIECE] = tail[:, core * W : (core + 1) * W]


def middle_of(both, side, small):
    return pl.pallas_call(
        middle_kernel,
        out_shape=[shape_of((NC * PIECE, W), BF16)] * SLOTS,
        compiler_params=params(12),
        cost_estimate=cost(2 * ROWS * D, 2 * 1024 * 1024),
    )(*both, *side, *small)


def add_kernel(mine, arrived, out):
    out[...] = (mine[...].astype(F32) + arrived[...].astype(F32)).astype(BF16)


def added(mine, arrived):
    return pl.pallas_call(
        add_kernel,
        out_shape=shape_of(mine.shape, BF16),
        compiler_params=params(8),
        cost_estimate=cost(2 * ROWS * D, 1024 * 1024),
    )(mine, arrived)


def chip_kernel(mine, arrived, own, other):
    total = arrived[...].astype(F32)
    total = total + jnp.where(lax.axis_index("c") == 0, jnp.zeros_like(total), mine[...].astype(F32))
    own[...] = total[:PIECE]
    other[...] = total[PIECE:]


def chip_of(mine, arrived):
    return pl.pallas_call(
        chip_kernel,
        out_shape=[shape_of((PIECE, W))] * 2,
        compiler_params=params(8),
        cost_estimate=cost(2 * ROWS * D, 1024 * 1024),
    )(mine, arrived)


def final_kernel(own, other, value_grad, gate_grad, out_grad, taps_grad, gain_grad):
    total = own[...] + other[...]
    value_grad[...] = total[:CUT]
    gate_grad[...] = total[CUT : 2 * CUT]
    out_grad[...] = total[2 * CUT : 3 * CUT]
    taps_grad[...] = total[3 * CUT : 3 * CUT + K]
    gain_grad[...] = total[3 * CUT + K :]


def final_of(own, other):
    part = shape_of((CUT, W))
    return pl.pallas_call(
        final_kernel,
        out_shape=[part, part, part, shape_of((K, W)), shape_of((1, W))],
        compiler_params=params(8),
        cost_estimate=cost(2 * ROWS * D, 1024 * 1024),
    )(own, other)


def share(by, slopes, others, both, lent):
    here = lax.axis_index("x")
    core = lax.axis_index("c")
    chip = lax.rem(here + by * (1 - 2 * core) + NX, NX)
    mine = both[pl.ds(pl.multiple_of((chip * NC + core) * BLOCK, BLOCK), BLOCK), :]
    theirs = lent[pl.ds(pl.multiple_of(chip * BLOCK, BLOCK), BLOCK), :]
    contract = (((1,), (1,)), ((), ()))
    total = lax.dot_general(slopes[...], mine, contract, preferred_element_type=F32)
    return total + lax.dot_general(others[...], theirs, contract, preferred_element_type=F32)


def far_kernel(slopes, others, both, lent, far, back):
    far[...] = share(2, slopes, others, both, lent).astype(BF16)
    back[...] = share(-1, slopes, others, both, lent).astype(BF16)


def near_kernel(slopes, others, both, lent, arrived, near):
    near[...] = (share(1, slopes, others, both, lent) + arrived[...].astype(F32)).astype(BF16)


def own_kernel(slopes, others, both, lent, first, second, out):
    total = share(0, slopes, others, both, lent)
    out[...] = (total + first[...].astype(F32) + second[...].astype(F32)).astype(BF16)


def share_call(kernel, count, shares, *args):
    piece = shape_of((ROWS, BLOCK), BF16)
    return pl.pallas_call(
        kernel,
        out_shape=[piece] * count,
        compiler_params=params(12),
        cost_estimate=cost(2 * ROWS * D * 256 * shares, shares * 2 * 1024 * 1024),
    )(*args)


def from_behind(value, by):
    count = lax.axis_size(SP)
    return lax.ppermute(value, SP, [(i, i + by) for i in range(count) if 0 <= i + by < count])


def to_slot(value, slot):
    pairs = [(t, (t // NC + slot // 2) % NX * NC + (t + slot) % NC) for t in range(NX * NC)]
    return lax.ppermute(value, TP, pairs)


def chip_sums(own):
    pair = own + to_slot(own, 1)
    return [pair] + [to_slot(pair, slot) for slot in (2, 6, 4)]


def along(value, by):
    pairs = [(t, (t // NC + (by if t % NC == 0 else -by)) % NX * NC + t % NC) for t in range(NX * NC)]
    return lax.ppermute(value, TP, pairs)


def further(value, axis, by):
    count = lax.axis_size(axis)
    return lax.ppermute(value, axis, [(i, (i + by) % count) for i in range(count)])


def spread(parts, axis, order):
    return [parts[0]] + [further(parts[by], axis, by) for by in order]


def round_z(value, cores):
    pairs = [(z * NC + c, (z + 1 - 2 * c) % NZ * NC + c) for z in range(NZ) for c in cores]
    return lax.ppermute(value, ("z", "c"), pairs)


def shards(block_input, value_proj, gate_proj, conv_taps, norm_gain, out_proj, grad_output):
    to_next, to_prior, both, out_side = edges(block_input, grad_output, value_proj, gate_proj, out_proj)
    prior = from_behind(to_next, 1)
    after = from_behind(to_prior, -1)
    mixed, sgate, factor = glu(block_input, both)
    conv, sums = conv_of(mixed, conv_taps)
    edge, sums = edge_conv_of(mixed, prior, after, conv_taps, sums)
    sums = chip_sums(sums)
    slope, lend = slopes_of(grad_output, out_side, both)
    normed, norm_slope, inverse, activated, back, gain_part = norm_of(
        conv, edge, slope, after, norm_gain.reshape(1, W), sums
    )
    back = chip_sums(back)
    other_activated = to_slot(activated, 1)
    out_parts = out_grad_of(grad_output, activated, other_activated)
    out_parts = spread(out_parts, "y", Y_ORDER)
    slopes, curve = adjoint_of(normed, norm_slope, inverse, back, conv_taps, sgate, factor)
    others = to_slot(slopes, 1)
    own_parts = own_weight_grad_of(block_input, slopes)
    both_parts = weight_grad_of(block_input, others, own_parts)
    both_parts = spread(both_parts, "y", Y_ORDER)
    lent = to_slot(lend, 1)
    sides = (slopes, others, both, lent)
    far, single = share_call(far_kernel, 2, 2, *sides)
    arrived = along(far, 1)
    (near,) = share_call(near_kernel, 1, 1, *sides, arrived)
    near = along(near, 1)
    single = along(single, -1)
    taps_part = taps_of(curve, mixed, prior, gain_part)
    other_taps = to_slot(taps_part, 1)
    small = spread([jnp.concatenate([taps_part, other_taps], axis=1)] * NY, "y", Y_ORDER)
    parts = middle_of(both_parts, out_parts, small)
    arrived = round_z(parts[0], (0,))
    for slot in (3, 2, 1):
        passed = added(parts[slot], arrived)
        arrived = round_z(passed, (0, 1))
    own, other = chip_of(parts[0], arrived)
    other = to_slot(other, 1)
    (input_grad,) = share_call(own_kernel, 1, 1, *sides, near, single)
    value_grad, gate_grad, out_grad, taps_grad, gain_grad = final_of(own, other)
    return (input_grad, value_grad, gate_grad, out_grad, taps_grad, gain_grad.reshape(W))


Y_ORDER = (2, 1, 3)


def solution(mesh):
    finer = Mesh(mesh.devices.reshape(NZ, NY, NX, NC), ("z", "y", "x", "c"))
    placed = (P(SP, None), P(None, TP), P(None, TP), P(None, TP), P(TP), P(None, TP), P(SP, None))
    split = P(SP, TP)
    return jax.shard_map(
        shards,
        mesh=finer,
        in_specs=placed,
        out_specs=(split, split, split, split, P(None, TP), P(TP)),
        check_vma=False,
    )
```

```python
import jax
import jax.numpy as jnp
from jax import lax
from jax.experimental import pallas as pl
from jax.experimental.pallas import tpu as pltpu
from jax.sharding import Mesh
from jax.sharding import PartitionSpec as P


SP = ("z", "y")
TP = ("x", "c")
NZ, NY, NX, NC = 8, 4, 4, 2
C = 1024
D = 2048
K = 31
ROWS = 1024
W = 128
PAD = 32
EXT = ROWS + PAD
BLOCK = D // 8
SLOTS = NZ // NC
PART = D // (NY * NC)
CUT = D // (NY * NZ)
PIECE = 3 * CUT + K + 1
FLOOR = 0.1
F32 = jnp.float32
BF16 = jnp.bfloat16


def params(mib, **more):
    return pltpu.CompilerParams(vmem_limit_bytes=mib * 1024 * 1024, **more)


def cost(flops, size):
    return pl.CostEstimate(flops=flops, bytes_accessed=size, transcendentals=0)


def dot(a, b):
    return jnp.dot(a, b, preferred_element_type=F32)


def shape_of(shape, dtype=F32):
    return jax.ShapeDtypeStruct(shape, dtype)


def edge_kernel(
    rows, grads, value_proj, gate_proj, out_proj, to_next, to_prior, both, out_side, ends, grad_head, sems
):
    pairs = [
        (rows.at[:PAD], ends.at[:PAD]),
        (rows.at[ROWS - PAD :], ends.at[PAD:]),
        (value_proj, both.at[:, :W]),
        (gate_proj, both.at[:, W:]),
        (grads.at[:PAD], grad_head),
        (out_proj, out_side),
    ]
    copies = [pltpu.make_async_copy(a, b, sems.at[i]) for i, (a, b) in enumerate(pairs)]
    for copy in copies:
        copy.start()
    for copy in copies[:4]:
        copy.wait()
    both_parts = dot(ends[...], both[...])
    mixed = (both_parts[:, :W] * jax.nn.sigmoid(both_parts[:, W:])).astype(BF16).astype(F32)
    to_prior[:PAD] = mixed[:PAD]
    to_next[...] = mixed[PAD:]
    for copy in copies[4:]:
        copy.wait()
    to_prior[PAD:] = dot(grad_head[...], out_side[...])


def in_hbm(value):
    return pltpu.with_memory_space_constraint(value, pltpu.HBM)


def edges(block_input, grad_output, value_proj, gate_proj, out_proj):
    hbm = pl.BlockSpec(memory_space=pltpu.HBM)
    vmem = pl.BlockSpec(memory_space=pltpu.VMEM)
    args = [in_hbm(v) for v in (block_input, grad_output, value_proj, gate_proj, out_proj)]
    return pl.pallas_call(
        edge_kernel,
        in_specs=[hbm] * 5,
        out_specs=[vmem] * 4,
        out_shape=[shape_of((PAD, W)), shape_of((2 * PAD, W)), shape_of((D, 2 * W), BF16), shape_of((D, W), BF16)],
        scratch_shapes=[
            pltpu.VMEM((2 * PAD, D), BF16),
            pltpu.VMEM((PAD, D), BF16),
            pltpu.SemaphoreType.DMA((6,)),
        ],
        compiler_params=params(8),
        cost_estimate=cost(2 * 96 * D * 256, 2 * 1024 * 1024),
    )(*args)


def glu_kernel(rows, both, mixed, sgate, factor):
    step = 256
    for r in range(0, ROWS, step):
        parts = dot(rows[r : r + step, :], both[...])
        value = parts[:, :W]
        gate = jax.nn.sigmoid(parts[:, W:])
        mixed[r : r + step, :] = (value * gate).astype(BF16).astype(F32)
        sgate[r : r + step, :] = gate
        factor[r : r + step, :] = value * gate * (1.0 - gate)


def glu(block_input, both):
    return pl.pallas_call(
        glu_kernel,
        out_shape=[shape_of((ROWS, W))] * 3,
        compiler_params=params(12),
        cost_estimate=cost(2 * ROWS * D * 256, 7 * 1024 * 1024),
    )(block_input, both)


def slope_kernel(rows, out_side, both, slope, lend, sems):
    core = lax.axis_index("c")
    copies = []
    for x in range(NX):
        at = pl.multiple_of((x * NC + 1 - core) * BLOCK, BLOCK)
        copies.append(
            pltpu.make_async_copy(
                both.at[pl.ds(at, BLOCK), :], lend.at[x * BLOCK : (x + 1) * BLOCK, :], sems.at[x]
            )
        )
        copies[-1].start()
    slope[...] = dot(rows[...], out_side[...])
    for copy in copies:
        copy.wait()


def slopes_of(grad_output, out_side, both):
    vmem = pl.BlockSpec(memory_space=pltpu.VMEM)
    return pl.pallas_call(
        slope_kernel,
        in_specs=[vmem] * 3,
        out_specs=[vmem] * 2,
        out_shape=[shape_of((ROWS, W)), shape_of((NX * BLOCK, 2 * W), BF16)],
        scratch_shapes=[pltpu.SemaphoreType.DMA((NX,))],
        compiler_params=params(8),
        cost_estimate=cost(2 * ROWS * D * 256, 5 * 1024 * 1024),
    )(grad_output, out_side, both)


def store_sums(out, value, other):
    out[0, :] = jnp.sum(value, axis=1)
    out[1, :] = jnp.sum(other, axis=1)


def spread_sums(parts, outs):
    total = (parts[0][...] + parts[1][...]) + (parts[2][...] + parts[3][...])
    step = 96
    for row, out in enumerate(outs):
        mean = total[row : row + 1, :] * (1.0 / C)
        for r in range(0, EXT, step):
            out[r : r + step, :] = jnp.broadcast_to(mean[:, r : r + step], (W, step)).T


def swept(source, taps, base, step, shifts):
    total = jnp.zeros((step, W), F32)
    for residue in range(8):
        ks = [k for k in range(K) if shifts(k) % 8 == residue]
        low = min(shifts(k) for k in ks)
        high = max(shifts(k) for k in ks)
        block = source[pl.ds(base + low, step + high - low), :]
        for k in ks:
            at = shifts(k) - low
            total = total + taps[k : k + 1, :] * block[at : at + step]
    return total


def conv_kernel(mixed, taps, conv, sums, history):
    history[:PAD] = jnp.zeros((PAD, W), F32)
    history[PAD:] = mixed[...]
    step = 128

    def body(i, carry):
        base = pl.multiple_of(i * step, step)
        conv[pl.ds(base, step), :] = swept(history, taps, base, step, lambda k: PAD - k)
        return carry

    lax.fori_loop(0, ROWS // step, body, 0)
    value = conv[...]
    store_sums(sums, value, value * value)


def conv_of(mixed, taps):
    return pl.pallas_call(
        conv_kernel,
        out_shape=[shape_of((ROWS, W)), shape_of((2, ROWS))],
        scratch_shapes=[pltpu.VMEM((PAD + ROWS, W), F32)],
        compiler_params=params(12),
        cost_estimate=cost(2 * ROWS * D * 128, 2 * 1024 * 1024),
    )(mixed, taps)


def edge_conv_kernel(mixed, prior, after, taps, main_sums, edge, sums, low, high):
    low[:PAD] = prior[...]
    low[PAD:] = mixed[:PAD]
    high[:PAD] = mixed[ROWS - PAD :]
    high[PAD:] = after[:PAD]
    edge[:PAD] = swept(low, taps, 0, PAD, lambda k: PAD - k)
    edge[PAD:] = swept(high, taps, 0, PAD, lambda k: PAD - k)
    value = edge[...]
    sums[:, PAD:ROWS] = main_sums[:, PAD:]
    for row, term in enumerate((value, value * value)):
        ends = jnp.sum(term, axis=1)[None]
        sums[row : row + 1, :PAD] = ends[:, :PAD]
        sums[row : row + 1, ROWS:] = ends[:, PAD:]


def edge_conv_of(mixed, prior, after, taps, main_sums):
    return pl.pallas_call(
        edge_conv_kernel,
        out_shape=[shape_of((2 * PAD, W)), shape_of((2, EXT))],
        scratch_shapes=[pltpu.VMEM((2 * PAD, W), F32)] * 2,
        compiler_params=params(8),
        cost_estimate=cost(2 * ROWS * D * 16, 1024 * 1024),
    )(mixed, prior, after, taps, main_sums)


def norm_kernel(
    main, edge, slope, after, gain, s0, s1, s2, s3, normed, norm_slope, inverse, activated, back, gain_part,
    centers, squares,
):
    normed[:PAD] = edge[:PAD]
    normed[PAD:ROWS] = main[PAD:]
    normed[ROWS:] = edge[PAD:]
    spread_sums((s0, s1, s2, s3), (centers, squares))
    center = centers[...]
    inv = lax.rsqrt(squares[...] - center * center + FLOOR)
    norm = (normed[...] - center) * inv
    inverse[...] = inv
    normed[...] = norm
    scale = gain[...]
    scaled = norm * scale
    squash = jax.nn.sigmoid(scaled)
    activated[...] = (scaled * squash)[:ROWS].astype(BF16)
    bend = squash * (1.0 + scaled * (1.0 - squash))
    own = slope[...] * bend[:ROWS]
    gain_part[...] = jnp.sum(own * norm[:ROWS], axis=0, keepdims=True)
    own = own * scale
    past = after[PAD:] * bend[ROWS:] * scale
    norm_slope[:ROWS] = own
    norm_slope[ROWS:] = past
    value = norm_slope[...]
    store_sums(back, value, value * norm)


def norm_of(main, edge, slope, after, gain, sums):
    ext = shape_of((EXT, W))
    return pl.pallas_call(
        norm_kernel,
        out_shape=[ext, ext, ext, shape_of((ROWS, W), BF16), shape_of((2, EXT)), shape_of((1, W))],
        scratch_shapes=[pltpu.VMEM((EXT, W), F32)] * 2,
        compiler_params=params(16),
        cost_estimate=cost(2 * ROWS * D * 128, 2 * 1024 * 1024),
    )(main, edge, slope, after, gain, *sums)


def adjoint_kernel(
    normed, norm_slope, inverse, s0, s1, s2, s3, taps, sgate, factor, slopes, curve, means, crosses
):
    spread_sums((s0, s1, s2, s3), (means, crosses))
    curve[...] = inverse[...] * (norm_slope[...] - means[...] - normed[...] * crosses[...])

    @pl.when((lax.axis_index("z") == NZ - 1) & (lax.axis_index("y") == NY - 1))
    def _():
        curve[ROWS:] = jnp.zeros((PAD, W), F32)

    step = 128

    def spread(i, carry):
        base = pl.multiple_of(i * step, step)
        total = swept(curve, taps, base, step, lambda k: k)
        slopes[pl.ds(base, step), :W] = (total * sgate[pl.ds(base, step), :]).astype(BF16)
        slopes[pl.ds(base, step), W:] = (total * factor[pl.ds(base, step), :]).astype(BF16)
        return carry

    lax.fori_loop(0, ROWS // step, spread, 0)


def adjoint_of(normed, norm_slope, inverse, back, taps, sgate, factor):
    return pl.pallas_call(
        adjoint_kernel,
        out_shape=[shape_of((ROWS, 2 * W), BF16), shape_of((EXT, W))],
        scratch_shapes=[pltpu.VMEM((EXT, W), F32)] * 2,
        compiler_params=params(16),
        cost_estimate=cost(2 * ROWS * D * 256, 2 * 1024 * 1024),
    )(normed, norm_slope, inverse, *back, taps, sgate, factor)


def taps_kernel(curve, mixed, prior, gain_part, taps_part, history):
    history[:PAD] = prior[...]
    history[PAD:] = mixed[...]
    inner = 64

    def gather(i, sums):
        base = pl.multiple_of(i * inner, inner)
        now = curve[pl.ds(base, inner), :]
        sums = list(sums)
        for residue in range(8):
            ks = [k for k in range(K) if (PAD - k) % 8 == residue]
            low, high = PAD - max(ks), PAD - min(ks)
            block = history[pl.ds(base + low, inner + high - low), :]
            for k in ks:
                at = PAD - k - low
                sums[k] = sums[k] + jnp.sum((now * block[at : at + inner]).reshape(inner // 8, 8, W), axis=0)
        return tuple(sums)

    sums = lax.fori_loop(0, ROWS // inner, gather, tuple(jnp.zeros((8, W), F32) for _ in range(K)))
    for k in range(K):
        taps_part[k : k + 1, :] = jnp.sum(sums[k], axis=0, keepdims=True)
    taps_part[K:, :] = gain_part[...]


def taps_of(curve, mixed, prior, gain_part):
    return pl.pallas_call(
        taps_kernel,
        out_shape=shape_of((K + 1, W)),
        scratch_shapes=[pltpu.VMEM((PAD + ROWS, W), F32)],
        compiler_params=params(8),
        cost_estimate=cost(2 * ROWS * D * 64, 1024 * 1024),
    )(curve, mixed, prior, gain_part)


def kept_by(slot):
    core = lax.axis_index("c")
    by = 4 * (1 - core) if slot == 0 else slot * (1 - 2 * core) + NZ
    return lax.rem(lax.axis_index("z") + by, NZ)


def across(rows, side, parts, lanes):
    step = D // NZ
    for slot in range(SLOTS):
        at = pl.multiple_of(kept_by(slot) * step, step)
        part = lax.dot_general(
            rows[:, pl.ds(at, step)], side, (((0,), (0,)), ((), ())), preferred_element_type=F32
        )
        parts[:, slot * CUT : (slot + 1) * CUT, lanes] = part.astype(BF16).reshape(NY, CUT, side.shape[1])


def along_y(by):
    return lax.rem(lax.axis_index("y") + by, NY)


def out_grad_kernel(rows, activated, other, *rest):
    outs, parts = rest[:NY], rest[NY]
    across(rows, activated[...], parts, slice(0, W))
    across(rows, other[...], parts, slice(W, 2 * W))
    for by, out in enumerate(outs):
        out[...] = parts[along_y(by)]


def out_grad_of(grad_output, activated, other):
    return pl.pallas_call(
        out_grad_kernel,
        out_shape=[shape_of((PART, 2 * W), BF16)] * NY,
        scratch_shapes=[pltpu.VMEM((NY, PART, 2 * W), BF16)],
        compiler_params=params(8),
        cost_estimate=cost(2 * ROWS * D * 256, 5 * 1024 * 1024),
    )(grad_output, activated, other)


def own_weight_grad_kernel(rows, slopes, parts):
    across(rows, slopes[...], parts, slice(0, 2 * W))


def own_weight_grad_of(block_input, slopes):
    return pl.pallas_call(
        own_weight_grad_kernel,
        out_shape=shape_of((NY, PART, 2 * W), BF16),
        compiler_params=params(8),
        cost_estimate=cost(2 * ROWS * D * 128, 3 * 1024 * 1024),
    )(block_input, slopes)


def weight_grad_kernel(rows, others, own, *rest):
    outs, parts = rest[:NY], rest[NY]
    across(rows, others[...], parts, slice(0, 2 * W))
    for by, out in enumerate(outs):
        out[:, : 2 * W] = own[along_y(by)]
        out[:, 2 * W :] = parts[along_y(by)]


def weight_grad_of(block_input, others, own):
    return pl.pallas_call(
        weight_grad_kernel,
        out_shape=[shape_of((PART, 4 * W), BF16)] * NY,
        scratch_shapes=[pltpu.VMEM((NY, PART, 2 * W), BF16)],
        compiler_params=params(12),
        cost_estimate=cost(2 * ROWS * D * 128, 5 * 1024 * 1024),
    )(block_input, others, own)


def summed(parts):
    total = parts[0][...].astype(F32)
    for part in parts[1:]:
        total = total + part[...].astype(F32)
    return total


def middle_kernel(*refs):
    both, side, small, outs = refs[:NY], refs[NY : 2 * NY], refs[2 * NY : 3 * NY], refs[3 * NY :]
    total = summed(both).astype(BF16)
    outer = summed(side).astype(BF16)
    tail = summed(small).astype(BF16)
    for slot, out in enumerate(outs):
        rows = slice(slot * CUT, (slot + 1) * CUT)
        for core in range(NC):
            at, lane = core * PIECE, core * 2 * W
            out[at : at + CUT] = total[rows, lane : lane + W]
            out[at + CUT : at + 2 * CUT] = total[rows, lane + W : lane + 2 * W]
            out[at + 2 * CUT : at + 3 * CUT] = outer[rows, core * W : (core + 1) * W]
            out[at + 3 * CUT : at + PIECE] = tail[:, core * W : (core + 1) * W]


def middle_of(both, side, small):
    return pl.pallas_call(
        middle_kernel,
        out_shape=[shape_of((NC * PIECE, W), BF16)] * SLOTS,
        compiler_params=params(12),
        cost_estimate=cost(2 * ROWS * D, 2 * 1024 * 1024),
    )(*both, *side, *small)


def chip_kernel(mine, opposite, one, two, three, own, other):
    first = jnp.where(lax.axis_index("c") == 0, opposite[...].astype(F32), mine[...].astype(F32))
    total = first + summed((one, two, three))
    own[...] = total[:PIECE]
    other[...] = total[PIECE:]


def chip_of(mine, parts):
    return pl.pallas_call(
        chip_kernel,
        out_shape=[shape_of((PIECE, W))] * 2,
        compiler_params=params(8),
        cost_estimate=cost(2 * ROWS * D, 1024 * 1024),
    )(mine, *parts)


def final_kernel(own, other, value_grad, gate_grad, out_grad, taps_grad, gain_grad):
    total = own[...] + other[...]
    value_grad[...] = total[:CUT]
    gate_grad[...] = total[CUT : 2 * CUT]
    out_grad[...] = total[2 * CUT : 3 * CUT]
    taps_grad[...] = total[3 * CUT : 3 * CUT + K]
    gain_grad[...] = total[3 * CUT + K :]


def final_of(own, other):
    part = shape_of((CUT, W))
    return pl.pallas_call(
        final_kernel,
        out_shape=[part, part, part, shape_of((K, W)), shape_of((1, W))],
        compiler_params=params(8),
        cost_estimate=cost(2 * ROWS * D, 1024 * 1024),
    )(own, other)


def share(by, slopes, others, both, lent):
    here = lax.axis_index("x")
    core = lax.axis_index("c")
    chip = lax.rem(here + by * (1 - 2 * core) + NX, NX)
    mine = both[pl.ds(pl.multiple_of((chip * NC + core) * BLOCK, BLOCK), BLOCK), :]
    theirs = lent[pl.ds(pl.multiple_of(chip * BLOCK, BLOCK), BLOCK), :]
    contract = (((1,), (1,)), ((), ()))
    total = lax.dot_general(slopes[...], mine, contract, preferred_element_type=F32)
    return total + lax.dot_general(others[...], theirs, contract, preferred_element_type=F32)


def far_kernel(slopes, others, both, lent, far, back):
    far[...] = share(2, slopes, others, both, lent).astype(BF16)
    back[...] = share(-1, slopes, others, both, lent).astype(BF16)


def near_kernel(slopes, others, both, lent, arrived, near):
    near[...] = (share(1, slopes, others, both, lent) + arrived[...].astype(F32)).astype(BF16)


def own_kernel(slopes, others, both, lent, first, second, out):
    total = share(0, slopes, others, both, lent)
    out[...] = (total + first[...].astype(F32) + second[...].astype(F32)).astype(BF16)


def share_call(kernel, count, shares, *args):
    piece = shape_of((ROWS, BLOCK), BF16)
    return pl.pallas_call(
        kernel,
        out_shape=[piece] * count,
        compiler_params=params(12),
        cost_estimate=cost(2 * ROWS * D * 256 * shares, shares * 2 * 1024 * 1024),
    )(*args)


def from_behind(value, by):
    count = lax.axis_size(SP)
    return lax.ppermute(value, SP, [(i, i + by) for i in range(count) if 0 <= i + by < count])


def to_slot(value, slot):
    pairs = [(t, (t // NC + slot // 2) % NX * NC + (t + slot) % NC) for t in range(NX * NC)]
    return lax.ppermute(value, TP, pairs)


def chip_sums(own):
    pair = own + to_slot(own, 1)
    return [pair] + [to_slot(pair, slot) for slot in (2, 6, 4)]


def along(value, by):
    pairs = [(t, (t // NC + (by if t % NC == 0 else -by)) % NX * NC + t % NC) for t in range(NX * NC)]
    return lax.ppermute(value, TP, pairs)


def further(value, axis, by):
    count = lax.axis_size(axis)
    return lax.ppermute(value, axis, [(i, (i + by) % count) for i in range(count)])


def spread(parts, axis, order):
    return [parts[0]] + [further(parts[by], axis, by) for by in order]


def to_keeper(value, slot):
    if slot == 0:
        pairs = [(z * NC, (z + 4) % NZ * NC) for z in range(NZ)]
    else:
        pairs = [
            (z * NC + c, (z + (slot if c == 0 else -slot)) % NZ * NC + c) for z in range(NZ) for c in range(NC)
        ]
    return lax.ppermute(value, ("z", "c"), pairs)


def shards(block_input, value_proj, gate_proj, conv_taps, norm_gain, out_proj, grad_output):
    to_next, to_prior, both, out_side = edges(block_input, grad_output, value_proj, gate_proj, out_proj)
    prior = from_behind(to_next, 1)
    after = from_behind(to_prior, -1)
    mixed, sgate, factor = glu(block_input, both)
    conv, sums = conv_of(mixed, conv_taps)
    edge, sums = edge_conv_of(mixed, prior, after, conv_taps, sums)
    sums = chip_sums(sums)
    slope, lend = slopes_of(grad_output, out_side, both)
    normed, norm_slope, inverse, activated, back, gain_part = norm_of(
        conv, edge, slope, after, norm_gain.reshape(1, W), sums
    )
    back = chip_sums(back)
    other_activated = to_slot(activated, 1)
    out_parts = out_grad_of(grad_output, activated, other_activated)
    out_parts = spread(out_parts, "y", Y_ORDER)
    slopes, curve = adjoint_of(normed, norm_slope, inverse, back, conv_taps, sgate, factor)
    others = to_slot(slopes, 1)
    own_parts = own_weight_grad_of(block_input, slopes)
    both_parts = weight_grad_of(block_input, others, own_parts)
    both_parts = spread(both_parts, "y", Y_ORDER)
    lent = to_slot(lend, 1)
    sides = (slopes, others, both, lent)
    far, single = share_call(far_kernel, 2, 2, *sides)
    arrived = along(far, 1)
    (near,) = share_call(near_kernel, 1, 1, *sides, arrived)
    near = along(near, 1)
    single = along(single, -1)
    taps_part = taps_of(curve, mixed, prior, gain_part)
    other_taps = to_slot(taps_part, 1)
    small = spread([jnp.concatenate([taps_part, other_taps], axis=1)] * NY, "y", Y_ORDER)
    parts = middle_of(both_parts, out_parts, small)
    sent = {slot: to_keeper(parts[slot], slot) for slot in Z_ORDER}
    own, other = chip_of(parts[0], [sent[slot] for slot in range(SLOTS)])
    other = to_slot(other, 1)
    (input_grad,) = share_call(own_kernel, 1, 1, *sides, near, single)
    value_grad, gate_grad, out_grad, taps_grad, gain_grad = final_of(own, other)
    return (input_grad, value_grad, gate_grad, out_grad, taps_grad, gain_grad.reshape(W))


Y_ORDER = (2, 1, 3)
Z_ORDER = (0, 3, 2, 1)


def solution(mesh):
    finer = Mesh(mesh.devices.reshape(NZ, NY, NX, NC), ("z", "y", "x", "c"))
    placed = (P(SP, None), P(None, TP), P(None, TP), P(None, TP), P(TP), P(None, TP), P(SP, None))
    split = P(SP, TP)
    return jax.shard_map(
        shards,
        mesh=finer,
        in_specs=placed,
        out_specs=(split, split, split, split, P(None, TP), P(TP)),
        check_vma=False,
    )
```

```python
import functools

import jax
import jax.numpy as jnp
from jax import lax
from jax.experimental import pallas as pl
from jax.experimental.pallas import tpu as pltpu
from jax.sharding import Mesh
from jax.sharding import PartitionSpec as P


SP = ("z", "y")
TP = ("x", "c")
NZ, NY, NX, NC = 8, 4, 4, 2
C = 1024
D = 2048
K = 31
ROWS = 1024
W = 128
PAD = 32
EXT = ROWS + PAD
BLOCK = D // 8
SLOTS = NZ // NC
PART = D // (NY * NC)
CUT = D // (NY * NZ)
HALF = PART // 2
Y_ORDER = (2, 1, 3)
Z_ORDER = (0, 3, 2, 1)
PIECE = 3 * CUT + K + 1
FLOOR = 0.1
F32 = jnp.float32
BF16 = jnp.bfloat16


def params(mib, **more):
    return pltpu.CompilerParams(vmem_limit_bytes=mib * 1024 * 1024, **more)


def cost(flops, size):
    return pl.CostEstimate(flops=flops, bytes_accessed=size, transcendentals=0)


def dot(a, b):
    return jnp.dot(a, b, preferred_element_type=F32)


def shape_of(shape, dtype=F32):
    return jax.ShapeDtypeStruct(shape, dtype)


def edge_kernel(
    rows, grads, value_proj, gate_proj, out_proj, to_next, to_prior, both, out_side, ends, grad_head, sems
):
    pairs = [
        (rows.at[:PAD], ends.at[:PAD]),
        (rows.at[ROWS - PAD :], ends.at[PAD:]),
        (value_proj, both.at[:, :W]),
        (gate_proj, both.at[:, W:]),
        (grads.at[:PAD], grad_head),
        (out_proj, out_side),
    ]
    copies = [pltpu.make_async_copy(a, b, sems.at[i]) for i, (a, b) in enumerate(pairs)]
    for copy in copies:
        copy.start()
    for copy in copies[:4]:
        copy.wait()
    both_parts = dot(ends[...], both[...])
    mixed = (both_parts[:, :W] * jax.nn.sigmoid(both_parts[:, W:])).astype(BF16).astype(F32)
    to_prior[:PAD] = mixed[:PAD]
    to_next[...] = mixed[PAD:]
    for copy in copies[4:]:
        copy.wait()
    to_prior[PAD:] = dot(grad_head[...], out_side[...])


def in_hbm(value):
    return pltpu.with_memory_space_constraint(value, pltpu.HBM)


def edges(block_input, grad_output, value_proj, gate_proj, out_proj):
    hbm = pl.BlockSpec(memory_space=pltpu.HBM)
    vmem = pl.BlockSpec(memory_space=pltpu.VMEM)
    args = [in_hbm(v) for v in (block_input, grad_output, value_proj, gate_proj, out_proj)]
    return pl.pallas_call(
        edge_kernel,
        in_specs=[hbm] * 5,
        out_specs=[vmem] * 4,
        out_shape=[shape_of((PAD, W)), shape_of((2 * PAD, W)), shape_of((D, 2 * W), BF16), shape_of((D, W), BF16)],
        scratch_shapes=[
            pltpu.VMEM((2 * PAD, D), BF16),
            pltpu.VMEM((PAD, D), BF16),
            pltpu.SemaphoreType.DMA((6,)),
        ],
        compiler_params=params(8),
        cost_estimate=cost(2 * 96 * D * 256, 2 * 1024 * 1024),
    )(*args)


def glu_kernel(rows, both, mixed, sgate, factor):
    step = 256
    for r in range(0, ROWS, step):
        parts = dot(rows[r : r + step, :], both[...])
        value = parts[:, :W]
        gate = jax.nn.sigmoid(parts[:, W:])
        mixed[r : r + step, :] = (value * gate).astype(BF16).astype(F32)
        sgate[r : r + step, :] = gate
        factor[r : r + step, :] = value * gate * (1.0 - gate)


def glu(block_input, both):
    return pl.pallas_call(
        glu_kernel,
        out_shape=[shape_of((ROWS, W))] * 3,
        compiler_params=params(12),
        cost_estimate=cost(2 * ROWS * D * 256, 7 * 1024 * 1024),
    )(block_input, both)


def slope_kernel(rows, out_side, both, slope, lend, sems):
    core = lax.axis_index("c")
    copies = []
    for x in range(NX):
        at = pl.multiple_of((x * NC + 1 - core) * BLOCK, BLOCK)
        copies.append(
            pltpu.make_async_copy(
                both.at[pl.ds(at, BLOCK), :], lend.at[x * BLOCK : (x + 1) * BLOCK, :], sems.at[x]
            )
        )
        copies[-1].start()
    slope[...] = dot(rows[...], out_side[...])
    for copy in copies:
        copy.wait()


def slopes_of(grad_output, out_side, both):
    vmem = pl.BlockSpec(memory_space=pltpu.VMEM)
    return pl.pallas_call(
        slope_kernel,
        in_specs=[vmem] * 3,
        out_specs=[vmem] * 2,
        out_shape=[shape_of((ROWS, W)), shape_of((NX * BLOCK, 2 * W), BF16)],
        scratch_shapes=[pltpu.SemaphoreType.DMA((NX,))],
        compiler_params=params(8),
        cost_estimate=cost(2 * ROWS * D * 256, 5 * 1024 * 1024),
    )(grad_output, out_side, both)


def store_sums(out, value, other):
    out[0, :] = jnp.sum(value, axis=1)
    out[1, :] = jnp.sum(other, axis=1)


def spread_sums(parts, outs):
    total = (parts[0][...] + parts[1][...]) + (parts[2][...] + parts[3][...])
    step = 96
    for row, out in enumerate(outs):
        mean = total[row : row + 1, :] * (1.0 / C)
        for r in range(0, EXT, step):
            out[r : r + step, :] = jnp.broadcast_to(mean[:, r : r + step], (W, step)).T


def swept(source, taps, base, step, shifts):
    total = jnp.zeros((step, W), F32)
    for residue in range(8):
        ks = [k for k in range(K) if shifts(k) % 8 == residue]
        low = min(shifts(k) for k in ks)
        high = max(shifts(k) for k in ks)
        block = source[pl.ds(base + low, step + high - low), :]
        for k in ks:
            at = shifts(k) - low
            total = total + taps[k : k + 1, :] * block[at : at + step]
    return total


def conv_kernel(mixed, taps, conv, sums, history):
    history[:PAD] = jnp.zeros((PAD, W), F32)
    history[PAD:] = mixed[...]
    step = 128

    def body(i, carry):
        base = pl.multiple_of(i * step, step)
        conv[pl.ds(base, step), :] = swept(history, taps, base, step, lambda k: PAD - k)
        return carry

    lax.fori_loop(0, ROWS // step, body, 0)
    value = conv[...]
    store_sums(sums, value, value * value)


def conv_of(mixed, taps):
    return pl.pallas_call(
        conv_kernel,
        out_shape=[shape_of((ROWS, W)), shape_of((2, ROWS))],
        scratch_shapes=[pltpu.VMEM((PAD + ROWS, W), F32)],
        compiler_params=params(12),
        cost_estimate=cost(2 * ROWS * D * 128, 2 * 1024 * 1024),
    )(mixed, taps)


def edge_conv_kernel(mixed, prior, after, taps, main_sums, edge, sums, low, high):
    low[:PAD] = prior[...]
    low[PAD:] = mixed[:PAD]
    high[:PAD] = mixed[ROWS - PAD :]
    high[PAD:] = after[:PAD]
    edge[:PAD] = swept(low, taps, 0, PAD, lambda k: PAD - k)
    edge[PAD:] = swept(high, taps, 0, PAD, lambda k: PAD - k)
    value = edge[...]
    sums[:, PAD:ROWS] = main_sums[:, PAD:]
    for row, term in enumerate((value, value * value)):
        ends = jnp.sum(term, axis=1)[None]
        sums[row : row + 1, :PAD] = ends[:, :PAD]
        sums[row : row + 1, ROWS:] = ends[:, PAD:]


def edge_conv_of(mixed, prior, after, taps, main_sums):
    return pl.pallas_call(
        edge_conv_kernel,
        out_shape=[shape_of((2 * PAD, W)), shape_of((2, EXT))],
        scratch_shapes=[pltpu.VMEM((2 * PAD, W), F32)] * 2,
        compiler_params=params(8),
        cost_estimate=cost(2 * ROWS * D * 16, 1024 * 1024),
    )(mixed, prior, after, taps, main_sums)


def norm_kernel(
    main, edge, slope, after, gain, s0, s1, s2, s3, normed, norm_slope, inverse, activated, back, gain_part,
    centers, squares,
):
    normed[:PAD] = edge[:PAD]
    normed[PAD:ROWS] = main[PAD:]
    normed[ROWS:] = edge[PAD:]
    spread_sums((s0, s1, s2, s3), (centers, squares))
    center = centers[...]
    inv = lax.rsqrt(squares[...] - center * center + FLOOR)
    norm = (normed[...] - center) * inv
    inverse[...] = inv
    normed[...] = norm
    scale = gain[...]
    scaled = norm * scale
    squash = jax.nn.sigmoid(scaled)
    activated[...] = (scaled * squash)[:ROWS].astype(BF16)
    bend = squash * (1.0 + scaled * (1.0 - squash))
    own = slope[...] * bend[:ROWS]
    gain_part[...] = jnp.sum(own * norm[:ROWS], axis=0, keepdims=True)
    own = own * scale
    past = after[PAD:] * bend[ROWS:] * scale
    norm_slope[:ROWS] = own
    norm_slope[ROWS:] = past
    value = norm_slope[...]
    store_sums(back, value, value * norm)


def norm_of(main, edge, slope, after, gain, sums):
    ext = shape_of((EXT, W))
    return pl.pallas_call(
        norm_kernel,
        out_shape=[ext, ext, ext, shape_of((ROWS, W), BF16), shape_of((2, EXT)), shape_of((1, W))],
        scratch_shapes=[pltpu.VMEM((EXT, W), F32)] * 2,
        compiler_params=params(16),
        cost_estimate=cost(2 * ROWS * D * 128, 2 * 1024 * 1024),
    )(main, edge, slope, after, gain, *sums)


def adjoint_kernel(
    normed, norm_slope, inverse, s0, s1, s2, s3, taps, sgate, factor, slopes, curve, means, crosses
):
    spread_sums((s0, s1, s2, s3), (means, crosses))
    curve[...] = inverse[...] * (norm_slope[...] - means[...] - normed[...] * crosses[...])

    @pl.when((lax.axis_index("z") == NZ - 1) & (lax.axis_index("y") == NY - 1))
    def _():
        curve[ROWS:] = jnp.zeros((PAD, W), F32)

    step = 128

    def spread(i, carry):
        base = pl.multiple_of(i * step, step)
        total = swept(curve, taps, base, step, lambda k: k)
        slopes[pl.ds(base, step), :W] = (total * sgate[pl.ds(base, step), :]).astype(BF16)
        slopes[pl.ds(base, step), W:] = (total * factor[pl.ds(base, step), :]).astype(BF16)
        return carry

    lax.fori_loop(0, ROWS // step, spread, 0)


def adjoint_of(normed, norm_slope, inverse, back, taps, sgate, factor):
    return pl.pallas_call(
        adjoint_kernel,
        out_shape=[shape_of((ROWS, 2 * W), BF16), shape_of((EXT, W))],
        scratch_shapes=[pltpu.VMEM((EXT, W), F32)] * 2,
        compiler_params=params(16),
        cost_estimate=cost(2 * ROWS * D * 256, 2 * 1024 * 1024),
    )(normed, norm_slope, inverse, *back, taps, sgate, factor)


def taps_kernel(curve, mixed, prior, gain_part, taps_part, history):
    history[:PAD] = prior[...]
    history[PAD:] = mixed[...]
    inner = 64

    def gather(i, sums):
        base = pl.multiple_of(i * inner, inner)
        now = curve[pl.ds(base, inner), :]
        sums = list(sums)
        for residue in range(8):
            ks = [k for k in range(K) if (PAD - k) % 8 == residue]
            low, high = PAD - max(ks), PAD - min(ks)
            block = history[pl.ds(base + low, inner + high - low), :]
            for k in ks:
                at = PAD - k - low
                sums[k] = sums[k] + jnp.sum((now * block[at : at + inner]).reshape(inner // 8, 8, W), axis=0)
        return tuple(sums)

    sums = lax.fori_loop(0, ROWS // inner, gather, tuple(jnp.zeros((8, W), F32) for _ in range(K)))
    for k in range(K):
        taps_part[k : k + 1, :] = jnp.sum(sums[k], axis=0, keepdims=True)
    taps_part[K:, :] = gain_part[...]


def taps_of(curve, mixed, prior, gain_part):
    return pl.pallas_call(
        taps_kernel,
        out_shape=shape_of((K + 1, W)),
        scratch_shapes=[pltpu.VMEM((PAD + ROWS, W), F32)],
        compiler_params=params(8),
        cost_estimate=cost(2 * ROWS * D * 64, 1024 * 1024),
    )(curve, mixed, prior, gain_part)


def kept_by(slot):
    core = lax.axis_index("c")
    by = 4 * (1 - core) if slot == 0 else slot * (1 - 2 * core) + NZ
    return lax.rem(lax.axis_index("z") + by, NZ)


def across(rows, side, parts, lanes):
    step = D // NZ
    for i, slot in enumerate(Z_ORDER):
        at = pl.multiple_of(kept_by(slot) * step, step)
        part = lax.dot_general(
            rows[:, pl.ds(at, step)], side, (((0,), (0,)), ((), ())), preferred_element_type=F32
        )
        parts[:, i * CUT : (i + 1) * CUT, lanes] = part.astype(BF16).reshape(NY, CUT, side.shape[1])


def along_y(by):
    return lax.rem(lax.axis_index("y") + by, NY)


def out_grad_kernel(rows, activated, other, *rest):
    outs, parts = rest[:NY], rest[NY]
    across(rows, activated[...], parts, slice(0, W))
    across(rows, other[...], parts, slice(W, 2 * W))
    for by, out in enumerate(outs):
        out[...] = parts[along_y(by)]


def out_grad_of(grad_output, activated, other):
    return pl.pallas_call(
        out_grad_kernel,
        out_shape=[shape_of((PART, 2 * W), BF16)] * NY,
        scratch_shapes=[pltpu.VMEM((NY, PART, 2 * W), BF16)],
        compiler_params=params(8),
        cost_estimate=cost(2 * ROWS * D * 256, 5 * 1024 * 1024),
    )(grad_output, activated, other)


def own_weight_grad_kernel(rows, slopes, parts):
    across(rows, slopes[...], parts, slice(0, 2 * W))


def own_weight_grad_of(block_input, slopes):
    return pl.pallas_call(
        own_weight_grad_kernel,
        out_shape=shape_of((NY, PART, 2 * W), BF16),
        compiler_params=params(8),
        cost_estimate=cost(2 * ROWS * D * 128, 3 * 1024 * 1024),
    )(block_input, slopes)


def weight_grad_kernel(rows, others, own, taps_part, other_taps, *rest):
    firsts, seconds, parts = rest[:NY], rest[NY : 2 * NY], rest[2 * NY]
    across(rows, others[...], parts, slice(0, 2 * W))
    half = (K + 1) // 2
    small = (taps_part[:half], taps_part[half:], other_taps[:half], other_taps[half:])
    small = jnp.concatenate([part.astype(BF16) for part in small], axis=1)
    for by in range(NY):
        mine, theirs = own[along_y(by)], parts[along_y(by)]
        firsts[by][:HALF, : 2 * W] = mine[:HALF]
        firsts[by][:HALF, 2 * W :] = theirs[:HALF]
        firsts[by][HALF:] = small
        seconds[by][:, : 2 * W] = mine[HALF:]
        seconds[by][:, 2 * W :] = theirs[HALF:]


def weight_grad_of(block_input, others, own, taps_part, other_taps):
    first = shape_of((HALF + (K + 1) // 2, 4 * W), BF16)
    return pl.pallas_call(
        weight_grad_kernel,
        out_shape=[first] * NY + [shape_of((HALF, 4 * W), BF16)] * NY,
        scratch_shapes=[pltpu.VMEM((NY, PART, 2 * W), BF16)],
        compiler_params=params(12),
        cost_estimate=cost(2 * ROWS * D * 128, 5 * 1024 * 1024),
    )(block_input, others, own, taps_part, other_taps)


def summed(parts):
    total = parts[0][...].astype(F32)
    for part in parts[1:]:
        total = total + part[...].astype(F32)
    return total


def middle_kernel(low, *refs):
    both, side, small, outs = refs[:NY], refs[NY : 2 * NY], refs[2 * NY : 3 * NY], refs[3 * NY :]
    total = summed([part.at[:HALF] for part in both]).astype(BF16)
    outer = summed([part.at[low : low + HALF] for part in side]).astype(BF16)
    tail = summed([part.at[HALF:] for part in small]).astype(BF16)
    half = (K + 1) // 2
    for i, out in enumerate(outs):
        rows = slice(i * CUT, (i + 1) * CUT)
        for core in range(NC):
            at, lane = core * PIECE, core * 2 * W
            out[at : at + CUT] = total[rows, lane : lane + W]
            out[at + CUT : at + 2 * CUT] = total[rows, lane + W : lane + 2 * W]
            out[at + 2 * CUT : at + 3 * CUT] = outer[rows, core * W : (core + 1) * W]
            out[at + 3 * CUT : at + 3 * CUT + half] = tail[:, lane : lane + W]
            out[at + 3 * CUT + half : at + PIECE] = tail[:, lane + W : lane + 2 * W]


def middle_of(low, both, side, small):
    return pl.pallas_call(
        functools.partial(middle_kernel, low),
        out_shape=[shape_of((NC * PIECE, W), BF16)] * 2,
        compiler_params=params(12),
        cost_estimate=cost(2 * ROWS * D, 2 * 1024 * 1024),
    )(*both, *side, *small)


def chip_kernel(mine, opposite, one, two, three, own, other):
    first = jnp.where(lax.axis_index("c") == 0, opposite[...].astype(F32), mine[...].astype(F32))
    total = first + summed((one, two, three))
    own[...] = total[:PIECE]
    other[...] = total[PIECE:]


def chip_of(mine, parts):
    return pl.pallas_call(
        chip_kernel,
        out_shape=[shape_of((PIECE, W))] * 2,
        compiler_params=params(8),
        cost_estimate=cost(2 * ROWS * D, 1024 * 1024),
    )(mine, *parts)


def final_kernel(own, other, value_grad, gate_grad, out_grad, taps_grad, gain_grad):
    total = own[...] + other[...]
    value_grad[...] = total[:CUT]
    gate_grad[...] = total[CUT : 2 * CUT]
    out_grad[...] = total[2 * CUT : 3 * CUT]
    taps_grad[...] = total[3 * CUT : 3 * CUT + K]
    gain_grad[...] = total[3 * CUT + K :]


def final_of(own, other):
    part = shape_of((CUT, W))
    return pl.pallas_call(
        final_kernel,
        out_shape=[part, part, part, shape_of((K, W)), shape_of((1, W))],
        compiler_params=params(8),
        cost_estimate=cost(2 * ROWS * D, 1024 * 1024),
    )(own, other)


def share(by, slopes, others, both, lent):
    here = lax.axis_index("x")
    core = lax.axis_index("c")
    chip = lax.rem(here + by * (1 - 2 * core) + NX, NX)
    mine = both[pl.ds(pl.multiple_of((chip * NC + core) * BLOCK, BLOCK), BLOCK), :]
    theirs = lent[pl.ds(pl.multiple_of(chip * BLOCK, BLOCK), BLOCK), :]
    contract = (((1,), (1,)), ((), ()))
    total = lax.dot_general(slopes[...], mine, contract, preferred_element_type=F32)
    return total + lax.dot_general(others[...], theirs, contract, preferred_element_type=F32)


def far_kernel(slopes, others, both, lent, far, back):
    far[...] = share(2, slopes, others, both, lent).astype(BF16)
    back[...] = share(-1, slopes, others, both, lent).astype(BF16)


def near_kernel(slopes, others, both, lent, arrived, near):
    near[...] = (share(1, slopes, others, both, lent) + arrived[...].astype(F32)).astype(BF16)


def own_kernel(slopes, others, both, lent, first, second, out):
    total = share(0, slopes, others, both, lent)
    out[...] = (total + first[...].astype(F32) + second[...].astype(F32)).astype(BF16)


def share_call(kernel, count, shares, *args):
    piece = shape_of((ROWS, BLOCK), BF16)
    return pl.pallas_call(
        kernel,
        out_shape=[piece] * count,
        compiler_params=params(12),
        cost_estimate=cost(2 * ROWS * D * 256 * shares, shares * 2 * 1024 * 1024),
    )(*args)


def from_behind(value, by):
    count = lax.axis_size(SP)
    return lax.ppermute(value, SP, [(i, i + by) for i in range(count) if 0 <= i + by < count])


def to_slot(value, slot):
    pairs = [(t, (t // NC + slot // 2) % NX * NC + (t + slot) % NC) for t in range(NX * NC)]
    return lax.ppermute(value, TP, pairs)


def chip_sums(own):
    pair = own + to_slot(own, 1)
    return [pair] + [to_slot(pair, slot) for slot in (2, 6, 4)]


def along(value, by):
    pairs = [(t, (t // NC + (by if t % NC == 0 else -by)) % NX * NC + t % NC) for t in range(NX * NC)]
    return lax.ppermute(value, TP, pairs)


def further(value, axis, by):
    count = lax.axis_size(axis)
    return lax.ppermute(value, axis, [(i, (i + by) % count) for i in range(count)])


def spread(parts, axis, order):
    return [parts[0]] + [further(parts[by], axis, by) for by in order]


def to_keeper(value, slot):
    if slot == 0:
        pairs = [(z * NC, (z + 4) % NZ * NC) for z in range(NZ)]
    else:
        pairs = [
            (z * NC + c, (z + (slot if c == 0 else -slot)) % NZ * NC + c) for z in range(NZ) for c in range(NC)
        ]
    return lax.ppermute(value, ("z", "c"), pairs)


def shards(block_input, value_proj, gate_proj, conv_taps, norm_gain, out_proj, grad_output):
    to_next, to_prior, both, out_side = edges(block_input, grad_output, value_proj, gate_proj, out_proj)
    prior = from_behind(to_next, 1)
    after = from_behind(to_prior, -1)
    mixed, sgate, factor = glu(block_input, both)
    conv, sums = conv_of(mixed, conv_taps)
    edge, sums = edge_conv_of(mixed, prior, after, conv_taps, sums)
    sums = chip_sums(sums)
    slope, lend = slopes_of(grad_output, out_side, both)
    normed, norm_slope, inverse, activated, back, gain_part = norm_of(
        conv, edge, slope, after, norm_gain.reshape(1, W), sums
    )
    back = chip_sums(back)
    other_activated = to_slot(activated, 1)
    out_parts = out_grad_of(grad_output, activated, other_activated)
    out_parts = spread(out_parts, "y", Y_ORDER)
    slopes, curve = adjoint_of(normed, norm_slope, inverse, back, conv_taps, sgate, factor)
    others = to_slot(slopes, 1)
    taps_part = taps_of(curve, mixed, prior, gain_part)
    other_taps = to_slot(taps_part, 1)
    own_parts = own_weight_grad_of(block_input, slopes)
    halves = weight_grad_of(block_input, others, own_parts, taps_part, other_taps)
    firsts = spread(halves[:NY], "y", Y_ORDER)
    seconds = spread(halves[NY:], "y", Y_ORDER)
    lent = to_slot(lend, 1)
    sides = (slopes, others, both, lent)
    far, single = share_call(far_kernel, 2, 2, *sides)
    arrived = along(far, 1)
    (near,) = share_call(near_kernel, 1, 1, *sides, arrived)
    near = along(near, 1)
    single = along(single, -1)
    parts = middle_of(0, firsts, out_parts, firsts)
    parts += middle_of(HALF, seconds, out_parts, firsts)
    sent = {slot: to_keeper(part, slot) for slot, part in zip(Z_ORDER, parts)}
    own, other = chip_of(parts[0], [sent[slot] for slot in range(SLOTS)])
    other = to_slot(other, 1)
    (input_grad,) = share_call(own_kernel, 1, 1, *sides, near, single)
    value_grad, gate_grad, out_grad, taps_grad, gain_grad = final_of(own, other)
    return (input_grad, value_grad, gate_grad, out_grad, taps_grad, gain_grad.reshape(W))


def solution(mesh):
    finer = Mesh(mesh.devices.reshape(NZ, NY, NX, NC), ("z", "y", "x", "c"))
    placed = (P(SP, None), P(None, TP), P(None, TP), P(None, TP), P(TP), P(None, TP), P(SP, None))
    split = P(SP, TP)
    return jax.shard_map(
        shards,
        mesh=finer,
        in_specs=placed,
        out_specs=(split, split, split, split, P(None, TP), P(TP)),
        check_vma=False,
    )
```
